32 devices in a mesh: sp: 8 (over z, x), tp: 4 (over y, core).
Axes of the slice: x: 2, y: 2, z: 4, core: 2. Of those that a mesh axis runs over, the one named last changes fastest.
Arguments:
- layer_input: bfloat16 [1024, 2048], P('sp'), may hold values from -6 to 6
- out_cot: bfloat16 [1024, 2048], P('sp'), may hold values from -6 to 6
- routes: int32 [1024, 2], P('sp'), may hold values from 0 to 7, all different within a row; in each aligned block of 128 rows (0 to 127, 128 to 255, ...) at most 64 rows name the same one
- route_weights: float32 [1024, 2], P('sp'), may hold values from 0.2 to 1
- gate_weights: bfloat16 [8, 2048, 1024], P('sp', None, 'tp'), may hold values from -0.125 to 0.125
- up_weights: bfloat16 [8, 2048, 1024], P('sp', None, 'tp'), may hold values from -0.125 to 0.125
- down_weights: bfloat16 [8, 1024, 2048], P('sp', 'tp'), may hold values from -0.1875 to 0.1875
- out_proj: bfloat16 [2048, 2048], P(None, 'tp'), may hold values from -0.125 to 0.125
- queries: bfloat16 [1024, 2048], P('sp', 'tp'), may hold values from -6 to 6
- keys: bfloat16 [1024, 2048], P('sp', 'tp'), may hold values from -6 to 6
- values: bfloat16 [1024, 2048], P('sp', 'tp'), may hold values from -6 to 6
- mixer_out: bfloat16 [1024, 2048], P('sp', 'tp'), may hold values from -6 to 6
- entry_states: float32 [8, 32, 64, 64], P('sp', 'tp'), may hold values from -6 to 6
Outputs:
- grad_gate: bfloat16 [8, 2048, 1024], P('sp', None, 'tp')
- grad_up: bfloat16 [8, 2048, 1024], P('sp', None, 'tp')
- grad_down: bfloat16 [8, 1024, 2048], P('sp', 'tp')
- grad_proj: float32 [2048, 2048], P('sp', 'tp')
- grad_queries: bfloat16 [1024, 2048], P('sp', 'tp')
- grad_keys: bfloat16 [1024, 2048], P('sp', 'tp')
- grad_values: bfloat16 [1024, 2048], P('sp', 'tp')
The draws below stay inside these ranges and needn't reach their ends.
Inputs may be any that keep to these rules, and one draw needn't show every extreme that they name: `routes`: in each aligned block of 128 rows no expert is named by more than 64 rows, a bound that some block reaches; the numbers of one row differ.
All inputs are finite; a program needn't handle non-finite values.
Results may differ from the reference program's by a relative error of at most 0.01.
Values may be sent and summed in bfloat16 or wider, within the bound.
A program may use at most 128 MiB of HBM per device.

```python
import math
import jax
import jax.numpy as jnp
import numpy as np
from jax import lax

D = 2048
FF = 1024
HEADS = 32
DK = 64
TOPK = 2
SPAN = 128
TOK_DEV = 128
TOKENS = 1024
EXPERTS = 8
CAP = 64
HV = 2048
N_SP = 8


def raised(array, stream_key, source, target, shards_of, factor):
    def block_of(dim):
        return (jnp.arange(array.shape[dim]) // (array.shape[dim] // shards_of)).reshape((-1,) + (1,) * (array.ndim - 1 - dim))

    near = jax.random.permutation(stream_key, shards_of)[block_of(target)]
    far = (block_of(target) + shards_of // 2) % shards_of
    return jnp.where((block_of(source) == near) | (block_of(source) == far), factor * array, array)


def block_levels(rng, extent, split, smallest, high):
    level, own = 1.0, jax.random.fold_in(rng, 6)
    for axis_at, parts in split:
        heights = jnp.exp(jax.random.uniform(jax.random.fold_in(own, axis_at), (parts,), jnp.float32, smallest / len(split), high / len(split)))
        level = level * jnp.repeat(heights, extent[axis_at] // parts).reshape([-1 if axis == axis_at else 1 for axis in range(len(extent))])
    return level


def routed_block(rng, own, number, rows, amount, top, limit, lean):
    sequence = jax.random.permutation(rng, amount)
    heavy_load, common = shares(amount, rows * top, limit, lean, True), shares(amount, rows * top, limit, lean, False)
    places = jnp.arange(amount)

    def named(tallies, turn):
        used = int((tallies > 0).sum())
        fixed = max(1, used // 4)
        moved = fixed + (places - fixed + turn * (used - fixed)) % max(1, amount - fixed)
        return jnp.zeros((amount,), jnp.int32).at[sequence[jnp.where(places < fixed, places, moved)]].set(jnp.asarray(tallies, jnp.int32))

    tallies = jnp.where(number % 4 == 0, named(heavy_load, number // 4), named(common, number - number // 4 - 1))
    mixed = jax.random.permutation(jax.random.fold_in(own, 3), amount)
    donor, receiver = mixed[0:amount // 2 * 2:2], mixed[1:amount // 2 * 2:2]
    slack = jnp.minimum(tallies[donor] - 1, limit - tallies[receiver]) // 2
    slack = jnp.where((donor == sequence[0]) | (receiver == sequence[0]) | (tallies[receiver] == 0), 0, jnp.maximum(slack, 0))
    moved = jax.random.randint(jax.random.fold_in(own, 4), (amount // 2,), 0, 1 << 20) % (slack + 1)
    tallies = tallies.at[donor].add(-moved).at[receiver].add(moved)
    members = jnp.searchsorted(jnp.cumsum(tallies), jnp.arange(rows * top), side="right").astype(jnp.int32)
    listing = members.reshape(top, rows).T
    listing = listing[jax.random.permutation(jax.random.fold_in(own, 1), rows)]
    turn = jax.random.randint(jax.random.fold_in(own, 2), (rows, 1), 0, top)
    return jnp.take_along_axis(listing, (jnp.arange(top)[None, :] + turn) % top, axis=1)


def shares(number_of, total, bound, skew, full):
    weights = [(1 << 20) // math.isqrt(grade ** skew) + 1 for grade in range(1, number_of + 1)]
    largest = bound if full else min(bound, max(-(-total // number_of), total * weights[0] // sum(weights)))
    least = 1 if total - largest >= number_of - 1 else 0
    counts, surplus = [largest] + [least] * (number_of - 1), total - largest - least * (number_of - 1)
    while surplus > 0:
        candidates = [i for i in range(1, number_of) if counts[i] < largest] or [i for i in range(1, number_of) if counts[i] < bound]
        whole, left = sum([weights[i] for i in candidates]), surplus
        for i in candidates:
            more = min(bound - counts[i], max(1, left * weights[i] // whole), surplus)
            counts[i] = counts[i] + more
            surplus = surplus - more
    return np.array(counts)


def noise(rng, shape, spread, limit, pieces=(), kind=jnp.bfloat16):
    drawn = jax.random.normal(rng, shape, jnp.float32) * spread
    if len(pieces) > 0:
        drawn = block_levels(rng, shape, pieces, -0.22, 0.18) * drawn
    return jnp.clip(drawn, min=-limit, max=limit).astype(kind)


def bell_draw_with(key, shape, scale, limit, split, heavy, held_as=jnp.bfloat16):
    values = scale * jax.random.normal(key, shape, jnp.float32)
    if split:
        values = values * block_levels(key, shape, split, -0.22, 0.18)
    return jnp.clip(raised(values, jax.random.fold_in(key, 3), *heavy), -limit, limit).astype(held_as)


def setup_inputs(seed: int = 0) -> dict:
    seeds = jax.random.split(jax.random.key(seed), 14)
    layer_input = noise(seeds[0], (TOKENS, D), 1.0, 6.0, ((0, 8),))
    out_cot = bell_draw_with(seeds[1], (TOKENS, D), 1.0, 6.0, ((0, 8),), (0, 1, 8, 2.0))
    routes_keys = jax.random.split(jax.random.fold_in(seeds[2], 1), TOKENS // TOK_DEV)
    routes_turns = jax.random.permutation(jax.random.fold_in(seeds[2], 3), TOKENS // TOK_DEV)
    routes = jax.vmap(lambda own, number: routed_block(jax.random.fold_in(seeds[2], 2), own, number, TOK_DEV, EXPERTS, TOPK, CAP, 1))(routes_keys, routes_turns).reshape((TOKENS, TOPK))
    route_weights = jnp.clip(0.2 + 0.8 * jax.random.uniform(seeds[3], (TOKENS, TOPK), jnp.float32) ** block_levels(seeds[3], (TOKENS, TOPK), ((0, 8),), -0.2, 0.2), 0.2, 1.0)
    gate_weights = noise(seeds[4], (EXPERTS, D, FF), D ** -0.5, 0.125, ((0, 8), (2, 4)))
    up_weights = noise(seeds[5], (EXPERTS, D, FF), D ** -0.5, 0.125, ((0, 8), (2, 4)))
    down_weights = noise(seeds[6], (EXPERTS, FF, D), FF ** -0.5, 0.1875, ((0, 8), (1, 4)))
    out_proj = noise(seeds[7], (D, HV), HV ** -0.5, 0.125, ((1, 4),))
    queries = noise(seeds[8], (TOKENS, HV), 1.0, 6.0, ((0, 8), (1, 4)))
    keys = noise(seeds[9], (TOKENS, HV), 1.0, 6.0, ((0, 8), (1, 4)))
    values = noise(seeds[10], (TOKENS, HV), 1.0, 6.0, ((0, 8), (1, 4)))
    mixer_out = noise(seeds[11], (TOKENS, HV), 1.0, 6.0, ((0, 8), (1, 4)))
    entry_states = noise(seeds[12], (N_SP, HEADS, DK, DK), 1.0, 6.0, ((0, 8), (1, 4)), jnp.float32)
    return dict(layer_input=layer_input, out_cot=out_cot, routes=routes, route_weights=route_weights, gate_weights=gate_weights, up_weights=up_weights, down_weights=down_weights, out_proj=out_proj, queries=queries, keys=keys, values=values, mixer_out=mixer_out, entry_states=entry_states)


def decay_rates(head_ids, head_count, token_count):
    half_count = head_count // 2
    fraction = jnp.minimum(head_ids, half_count) / half_count
    base_rate = jnp.exp((1.0 - fraction) * jnp.log(1.0 / 32.0) + fraction * jnp.log(1.0 / token_count))
    return base_rate * (1.0 + jnp.maximum(head_ids - half_count, 0.0) / half_count)

def position_norm(positions, head_rates):
    return jnp.sqrt(jnp.expm1(-2.0 * head_rates)[None, :] / jnp.expm1(-2.0 * head_rates[None, :] * (positions[:, None] + 1.0)))

def rounded(values):
    return lax.optimization_barrier(values.astype(jnp.bfloat16)).astype(jnp.float32)

def retention_grads(queries, keys, values, head_cot, entry_states, head_rates):
    span_count = TOKENS // SPAN
    per_segment = TOK_DEV // SPAN
    key_scale = DK ** (-0.5)
    span_shape = (span_count, SPAN, HEADS, DK)
    query_wide = queries.reshape(span_shape).astype(jnp.float32)
    key_wide = keys.reshape(span_shape).astype(jnp.float32)
    value_wide = values.reshape(span_shape).astype(jnp.float32)
    cot_wide = head_cot.reshape(span_shape).astype(jnp.float32)
    offsets = jnp.arange(SPAN).astype(jnp.float32)
    distance = offsets[:, None] - offsets[None, :]
    decay_mat = jnp.where(distance[None] >= 0, jnp.exp(-head_rates[:, None, None] * jnp.maximum(distance, 0.0)[None]), 0.0)
    fwd_weights = rounded(jnp.einsum('cihd,cjhd->chij', query_wide, key_wide) * key_scale * decay_mat[None])
    back_weights = rounded(jnp.einsum('cihd,cjhd->chij', cot_wide, value_wide) * decay_mat[None])
    tail_decay = jnp.exp(-head_rates[None, :] * (SPAN - 1.0 - offsets)[:, None])
    lead_decay = jnp.exp(-head_rates[None, :] * (offsets + 1.0)[:, None])
    span_decay = jnp.exp(-head_rates * SPAN)
    updates = key_scale * jnp.einsum('cjhd,cjhe->chde', key_wide * tail_decay[None, :, :, None], value_wide, precision=lax.Precision.HIGHEST)
    backs = jnp.einsum('cihd,cihe->chde', query_wide * lead_decay[None, :, :, None], cot_wide, precision=lax.Precision.HIGHEST)

    def forward(carried, inputs_c):
        update, span_index = inputs_c
        saved_state = entry_states[span_index // per_segment]
        current = jnp.where(span_index % per_segment == 0, saved_state, carried)
        return (span_decay[:, None, None] * current + update, current)
    start_state = jnp.zeros((HEADS, DK, DK), jnp.float32)
    _, fwd_states = lax.scan(forward, start_state, (updates, jnp.arange(span_count, dtype=jnp.int32)))

    def backward(carried, update):
        return (span_decay[:, None, None] * carried + update, carried)
    _, rev_states = lax.scan(backward, start_state, backs, reverse=True)
    grad_q = key_scale * jnp.einsum('chij,cjhd->cihd', back_weights, key_wide)
    grad_q = grad_q + lead_decay[None, :, :, None] * jnp.einsum('chde,cihe->cihd', fwd_states, cot_wide, precision=lax.Precision.HIGHEST)
    grad_k = jnp.einsum('chij,cihd->cjhd', back_weights, query_wide)
    grad_k = key_scale * (grad_k + tail_decay[None, :, :, None] * jnp.einsum('chde,cjhe->cjhd', rev_states, value_wide, precision=lax.Precision.HIGHEST))
    grad_v = jnp.einsum('chij,cihe->cjhe', fwd_weights, cot_wide)
    grad_v = grad_v + key_scale * tail_decay[None, :, :, None] * jnp.einsum('chde,cjhd->cjhe', rev_states, key_wide, precision=lax.Precision.HIGHEST)
    flat_shape = (TOKENS, HEADS * DK)
    return (grad_q.reshape(flat_shape).astype(jnp.bfloat16), grad_k.reshape(flat_shape).astype(jnp.bfloat16), grad_v.reshape(flat_shape).astype(jnp.bfloat16))

def reference(layer_input, out_cot, routes, route_weights, gate_weights, up_weights, down_weights, out_proj, queries, keys, values, mixer_out, entry_states):
    pair_total = TOKENS * TOPK
    per_block = TOK_DEV * TOPK
    slot_count = N_SP * CAP
    flat_routes = routes.reshape(-1)
    onehot = (flat_routes.reshape(N_SP, per_block, 1) == jnp.arange(EXPERTS, dtype=jnp.int32)[None, None, :]).astype(jnp.int32)
    earlier = jnp.cumsum(onehot, axis=1) - onehot
    placed = lax.optimization_barrier(jnp.sum(earlier * onehot, axis=2)).reshape(-1)
    block_id = jnp.arange(pair_total, dtype=jnp.int32) // per_block
    target = flat_routes * slot_count + block_id * CAP + placed
    owner_tok = jnp.arange(pair_total, dtype=jnp.int32) // TOPK
    slot_tok = jnp.full((EXPERTS * slot_count,), TOKENS, jnp.int32).at[target].set(owner_tok)
    slot_weight = jnp.zeros((EXPERTS * slot_count,), jnp.float32).at[target].set(route_weights.reshape(-1))
    blank_row = jnp.zeros((1, D), jnp.bfloat16)
    input_ext = jnp.concatenate([layer_input, blank_row], 0)
    cot_ext = jnp.concatenate([out_cot, blank_row], 0)

    def expert_step(accum, inputs_e):
        gate_w, up_w, down_w, row_ids, row_weight = inputs_e
        exp_rows = input_ext[row_ids]
        exp_cot = (row_weight[:, None] * cot_ext[row_ids].astype(jnp.float32)).astype(jnp.bfloat16)
        gate_pre = jnp.dot(exp_rows, gate_w, preferred_element_type=jnp.float32)
        up_pre = jnp.dot(exp_rows, up_w, preferred_element_type=jnp.float32)
        sigmoid_g = jax.nn.sigmoid(gate_pre)
        activated = (gate_pre * sigmoid_g * up_pre).astype(jnp.bfloat16)
        grad_down = jnp.dot(activated.T, exp_cot, preferred_element_type=jnp.float32).astype(jnp.bfloat16)
        d_act = jnp.dot(exp_cot, down_w.T, preferred_element_type=jnp.float32)
        d_gate = (d_act * up_pre * sigmoid_g * (1.0 + gate_pre * (1.0 - sigmoid_g))).astype(jnp.bfloat16)
        d_up = (d_act * gate_pre * sigmoid_g).astype(jnp.bfloat16)
        grad_gate = jnp.dot(exp_rows.T, d_gate, preferred_element_type=jnp.float32).astype(jnp.bfloat16)
        grad_up = jnp.dot(exp_rows.T, d_up, preferred_element_type=jnp.float32).astype(jnp.bfloat16)
        returned = jnp.dot(d_gate, gate_w.T, preferred_element_type=jnp.float32)
        returned = returned + jnp.dot(d_up, up_w.T, preferred_element_type=jnp.float32)
        return (accum.at[row_ids].add(rounded(returned)), (grad_gate, grad_up, grad_down))
    accum, expert_out = lax.scan(expert_step, jnp.zeros((TOKENS + 1, D), jnp.float32), (gate_weights, up_weights, down_weights, slot_tok.reshape(EXPERTS, slot_count), slot_weight.reshape(EXPERTS, slot_count)))
    grad_gate, grad_up, grad_down = expert_out
    mixer_cot = (out_cot.astype(jnp.float32) + accum[:TOKENS]).astype(jnp.bfloat16)
    grad_proj = jnp.dot(mixer_cot.T, mixer_out, preferred_element_type=jnp.float32)
    head_rates = decay_rates(jnp.arange(HEADS).astype(jnp.float32), HEADS, TOKENS)
    positions = jnp.arange(TOKENS).astype(jnp.float32)
    head_cot = jnp.dot(mixer_cot, out_proj, preferred_element_type=jnp.float32).reshape(TOKENS, HEADS, DK)
    head_cot = (head_cot * position_norm(positions, head_rates)[:, :, None]).astype(jnp.bfloat16)
    grad_q, grad_k, grad_v = retention_grads(queries, keys, values, head_cot, entry_states, head_rates)
    return (grad_gate, grad_up, grad_down, grad_proj, grad_q, grad_k, grad_v)
```

```python
import functools
import math

import jax
import jax.numpy as jnp
from jax import lax
from jax.experimental import pallas as pl
from jax.experimental.pallas import tpu as pltpu
from jax.sharding import PartitionSpec as P

DK = 64
SPAN = 128
MESH = pl.DeviceIdType.MESH
VMEM = pl.BlockSpec(memory_space=pltpu.VMEM)


WAVE = (1, 2, 4, 3, 5, 6, 7)
HOPS = (2, 4, 6)
NT = (((1,), (1,)), ((), ()))
TN = (((0,), (0,)), ((), ()))


def partner(me, k):
    for bit in (1, 2, 4):
        if k & bit:
            me = me + bit - 2 * bit * ((me // bit) % 2)
    return me


def wire(src, dst, send_sem, recv_sem, target):
    return pltpu.make_async_remote_copy(
        src_ref=src,
        dst_ref=dst,
        send_sem=send_sem,
        recv_sem=recv_sem,
        device_id=target,
        device_id_type=MESH,
    )


def send(src, dst, send_sem, recv_sem, target):
    copy = wire(src, dst, send_sem, recv_sem, target)
    copy.start()
    return copy


def greet(experts, me, tp, narrow):
    barrier = pltpu.get_barrier_semaphore()
    for k in range(1, experts):
        pl.semaphore_signal(
            barrier, inc=1, device_id={"sp": (me + k) % experts}, device_id_type=MESH
        )
    for k in range(1, narrow):
        pl.semaphore_signal(
            barrier, inc=1, device_id={"tp": (tp + k) % narrow}, device_id_type=MESH
        )
    return barrier, experts + narrow - 2


def rates_of(ids, total, tokens):
    half = total // 2
    ids = ids.astype(jnp.float32)
    fraction = jnp.minimum(ids, float(half)) * (1.0 / half)
    low, high = math.log(1.0 / 32.0), math.log(1.0 / tokens)
    base = jnp.exp((1.0 - fraction) * low + fraction * high)
    return base * (1.0 + jnp.maximum(ids - float(half), 0.0) * (1.0 / half))


def iota(shape, dim):
    return lax.broadcasted_iota(jnp.int32, shape, dim)


def dot(a, b, dims=None):
    if dims is None:
        dims = (((1,), (0,)), ((), ()))
    return lax.dot_general(a, b, dims, preferred_element_type=jnp.float32)


def mega_kernel(
    experts,
    narrow,
    routes,
    gains,
    rows_hbm,
    cot_hbm,
    gate_hbm,
    up_hbm,
    down_hbm,
    proj_hbm,
    query_hbm,
    key_hbm,
    value_hbm,
    out_hbm,
    entry_hbm,
    gg,
    gu,
    gd,
    grad_proj,
    grad_q,
    grad_k,
    grad_v,
    rows_in,
    cot_in,
    gate_w,
    up_w,
    down_w,
    gate_t,
    up_t,
    down_t,
    proj,
    query,
    key,
    value,
    entry,
    rows_s,
    cot_s,
    extra,
    rbuf,
    cbuf,
    place,
    share_w,
    act,
    dg,
    du,
    part,
    near_buf,
    side_out,
    side_in,
    far_out,
    back,
    mixer,
    all_out,
    all_mixer,
    state,
    given,
    all_state,
    l_in,
    s_sp, r_sp, s_y, r_y, s_c, r_c,
    s_n, r_n, s_s, r_s, s_f, r_f, s_g, r_g,
    s_r, r_r, s_m, r_m, s_h, r_h, s_b, r_b,
):
    me, tp = lax.axis_index("sp"), lax.axis_index("tp")
    core, row = tp % 2, tp // 2
    mate, across = tp + 1 - 2 * core, (tp + 2) % narrow
    mate_core = 1 - core
    tok, width = rows_in.shape
    share = rows_s.shape[0] // experts
    cap = share * narrow
    cols = width // narrow
    pcols = width // experts
    heads = query.shape[1] // DK
    bf = jnp.bfloat16
    f32 = jnp.float32
    xmate = partner(me, 1)

    all_state[...] = jnp.zeros_like(all_state)
    barrier, count = greet(experts, me, tp, narrow)
    loads = {}
    first_in = (
        (9, rows_hbm, rows_in),
        (10, cot_hbm, cot_in),
        (3, out_hbm, all_out.at[me]),
        (0, gate_hbm.at[0], gate_w),
        (1, up_hbm.at[0], up_w),
        (2, down_hbm.at[0], down_w),
        (5, query_hbm, query),
        (6, key_hbm, key),
        (7, value_hbm, value),
        (8, entry_hbm.at[0], entry),
    )
    lanes = 128
    width = rows_in.shape[1]
    blocks = width // lanes
    held_at = [
        (spot // narrow) // 2 + 2 * ((spot // narrow) % 2) + narrow * (spot % narrow)
        for spot in range(blocks)
    ]
    first_in = first_in + tuple(
        (
            11 + spot,
            proj_hbm.at[lanes * block : lanes * (block + 1)],
            proj.at[lanes * spot : lanes * (spot + 1)],
        )
        for spot, block in enumerate(held_at)
    )
    def fetch(some):
        for i, src, dst in some:
            loads[i] = pltpu.make_async_copy(src, dst, l_in.at[i])
            loads[i].start()

    fetch(first_in[:3])

    named = iota((tok, tok), 0)
    first, second = routes[0:1, :] == named, routes[1:2, :] == named
    hit = jnp.logical_or(first, second)
    before = jnp.where(iota((tok, tok), 0) < iota((tok, tok), 1), 1.0, 0.0).astype(bf)
    rank = dot(jnp.where(hit, 1.0, 0.0).astype(bf), before)
    spot = jnp.where(hit, rank, -1.0)
    place[...] = spot
    gain = jnp.where(first, gains[0:1, :], 0.0) + jnp.where(second, gains[1:2, :], 0.0)
    share_w[...] = gain

    def spread_rows(a):
        return jnp.broadcast_to(
            a[0:experts][:, None, :], (experts, share, tok)
        ).reshape(experts * share, tok)

    slot = (iota((experts * share, tok), 0) % share + share * tp).astype(f32)
    mask = jnp.where(spread_rows(spot) == slot, 1.0, 0.0)
    part_gain = jnp.sum(mask * spread_rows(gain), axis=1, keepdims=True)
    chosen = mask.astype(bf)
    loads[9].wait()
    loads[10].wait()
    rows_s[...] = dot(chosen, rows_in[...]).astype(bf)
    cot_s[...] = (part_gain * dot(chosen, cot_in[...])).astype(bf)
    near_slot = (iota((share, tok), 0) + share * across).astype(f32)
    near_mask = jnp.where(place[pl.ds(xmate, 1), :] == near_slot, 1.0, 0.0)
    near_gain = jnp.sum(near_mask * share_w[pl.ds(xmate, 1), :], axis=1, keepdims=True)
    near_chosen = near_mask.astype(bf)
    extra[0] = dot(near_chosen, rows_in[...]).astype(bf)
    extra[1] = (near_gain * dot(near_chosen, cot_in[...])).astype(bf)
    own_slot = iota((cap, tok), 0).astype(f32)
    own_mask = jnp.where(place[pl.ds(me, 1), :] == own_slot, 1.0, 0.0)
    own_gain = jnp.sum(own_mask * share_w[pl.ds(me, 1), :], axis=1, keepdims=True)
    own_chosen = own_mask.astype(bf)

    def piece(buf, origin, index):
        return buf.at[pl.ds(pl.multiple_of(origin * cap + index * share, share), share)]

    def block(buf, index):
        return buf.at[pl.ds(pl.multiple_of(index * share, share), share)]

    def hold(origin):
        return pl.ds(pl.multiple_of(origin * cap, cap), cap)

    def quarter(index):
        return pl.ds(pl.multiple_of(index * cols, cols), cols)

    fetch(first_in[3:6])
    pl.semaphore_wait(barrier, count)
    arrays = ((rows_s, rbuf), (cot_s, cbuf))
    far, side, near, relayed = {}, {}, {}, {}
    for k in WAVE:
        peer = partner(me, k)
        for a, (src, dst) in enumerate(arrays):
            far[a, k] = send(
                block(src, peer), piece(dst, me, tp), s_sp.at[a, k], r_sp.at[a, k], {"sp": peer}
            )
    for a, (_, dst) in enumerate(arrays):
        side[a, 1] = send(
            extra.at[a], piece(dst, me, across), s_y.at[a, 1], r_y.at[a, 1], {"sp": xmate}
        )
    rbuf[hold(me), :] = dot(own_chosen, rows_in[...]).astype(bf)
    cbuf[hold(me), :] = (own_gain * dot(own_chosen, cot_in[...])).astype(bf)
    loads[3].wait()
    mine_out = all_out.at[me]
    inner = jnp.logical_or(me // 2 == 1, me // 2 == 2)

    def lend(slot, block, hop):
        index = block ^ hop
        held = all_out.at[partner(me, block)]
        return wire(held, held, s_r.at[slot], r_r.at[index], {"sp": partner(me, hop)})

    lend(0, 0, 2).start()

    def landed(block):
        held = all_out.at[me]
        wire(held, held, s_r.at[0], r_r.at[block], {"sp": xmate}).wait_recv()


    def land(k):
        origin = partner(me, k)
        for a, (_, dst) in enumerate(arrays):
            far[a, k].wait_recv()
            held = piece(dst, origin, tp)
            if k > 1:
                side[a, k] = send(held, held, s_y.at[a, k], r_y.at[a, k], {"tp": across})
            near[a, k] = send(held, held, s_c.at[a, 0, k], r_c.at[a, 0, k], {"tp": mate})

    def relay(k):
        origin = partner(me, k)
        for a, (_, dst) in enumerate(arrays):
            side[a, k].wait_recv()
            held = piece(dst, origin, across)
            relayed[a, k] = send(held, held, s_c.at[a, 1, k], r_c.at[a, 1, k], {"tp": mate})

    parted = {}

    def chunk(ks):
        for k in ks:
            if k > 0:
                for a in range(2):
                    near[a, k].wait_recv()
                    relayed[a, k].wait_recv()
        size = len(ks) * cap
        at = pl.ds(pl.multiple_of(partner(me, ks[0]) // len(ks) * size, size), size)
        rows, cots = rbuf[at, :], cbuf[at, :]
        gate = dot(rows, gate_w[...])
        up = dot(rows, up_w[...])
        sig = jax.nn.sigmoid(gate)
        d_act = dot(cots, down_t[...])
        act[at, :] = (gate * sig * up).astype(bf)
        d_gate = (d_act * up * sig * (1.0 + gate * (1.0 - sig))).astype(bf)
        d_up = (d_act * gate * sig).astype(bf)
        dg[at, :] = d_gate
        du[at, :] = d_up
        sums = (dot(d_gate, gate_t[...]) + dot(d_up, up_t[...])).astype(bf)
        for spot, block in enumerate(held_at):
            part[at, lanes * spot : lanes * (spot + 1)] = sums[
                :, lanes * block : lanes * (block + 1)
            ]
        for k in ks:
            dest = partner(me, k)
            for half in range(2):
                parted[k, half] = send(
                    part.at[hold(dest), quarter(half * 2 + mate_core)],
                    near_buf.at[k, half],
                    s_n.at[k, half],
                    r_n.at[k, half],
                    {"tp": mate},
                )

    crossed, gone = {}, {}

    def cross(k):
        dest = partner(me, k)
        parted[k, 0].wait_recv()
        parted[k, 1].wait_recv()
        side_out[k] = (
            part[hold(dest), quarter(across)].astype(f32) + near_buf[k, 1 - row].astype(f32)
        ).astype(bf)
        crossed[k] = send(side_out.at[k], side_in.at[k], s_s.at[k], r_s.at[k], {"tp": across})

    def ship(k):
        dest = partner(me, k)
        crossed[k].wait_recv()
        done = (
            part[hold(dest), quarter(tp)].astype(f32)
            + near_buf[k, row].astype(f32)
            + side_in[k].astype(f32)
        ).astype(bf)
        if k == 0:
            back[me] = done
        else:
            far_out[k] = done
            gone[k] = send(far_out.at[k], back.at[me], s_f.at[k], r_f.at[k], {"sp": dest})

    def weight_grads(step):
        span = width // experts
        at = pl.ds(step * span, span)
        rows = rbuf[:, at]
        gg[at, :] = dot(rows, dg[...], TN).astype(bf)
        gu[at, :] = dot(rows, du[...], TN).astype(bf)
        gd[:, at] = dot(act[...], cbuf[:, at], TN).astype(bf)

    def crossout():
        landed(2)
        lend(1, 0, 1).start()
        lend(2, 2, 1).start()

        @pl.when(inner)
        def _():
            lend(3, 0, 6).start()
            lend(4, 2, 6).start()

    def returnout():
        @pl.when(inner)
        def _():
            landed(6)
            landed(4)
            lend(3 + 2, 6, 2).start()
            lend(3 + 3, 4, 2).start()

    fetch(first_in[6:])
    turned = jnp.transpose(place[...])
    lane = iota((tok, 2 * cap), 1)
    picks = jnp.concatenate(
        [
            jnp.where(
                jnp.where(lane < cap, turned[:, 2 * p : 2 * p + 1], turned[:, 2 * p + 1 : 2 * p + 2])
                == (lane % cap).astype(f32),
                1.0,
                0.0,
            ).astype(bf)
            for p in range(experts // 2)
        ],
        axis=1,
    )
    for i in (0, 1, 2):
        loads[i].wait()
    for tile in range(experts):
        at = slice(tile * pcols, (tile + 1) * pcols)
        gate_t[:, at] = jnp.transpose(gate_w[at, :])
        up_t[:, at] = jnp.transpose(up_w[at, :])
        down_t[at, :] = jnp.transpose(down_w[:, at])
    land(1)
    land(2)
    land(4)
    land(3)
    relay(2)
    land(5)
    relay(4)
    relay(3)
    land(6)
    land(7)
    crossout()
    relay(1)
    relay(5)
    chunk((0, 1, 2, 3))
    chunk((4, 5))
    relay(6)
    cross(4)
    cross(5)
    cross(2)
    cross(3)
    relay(7)
    chunk((6, 7))
    cross(6)
    cross(7)
    ship(4)
    ship(5)
    cross(1)
    cross(0)
    ship(2)
    ship(3)
    returnout()
    weight_grads(0)
    weight_grads(1)
    ship(6)
    weight_grads(2)
    ship(7)
    weight_grads(3)
    ship(1)
    weight_grads(4)
    ship(0)
    weight_grads(5)
    weight_grads(6)
    weight_grads(7)
    for k in WAVE:
        gone[k].wait_recv()
    slots = back[...].reshape(experts * cap, cols)
    gained = dot(picks, slots)
    for m in range(narrow):
        block = pl.multiple_of((narrow * m + 2 * core + row) * lanes, lanes)
        spot = pl.multiple_of(tp * cols + m * lanes, lanes)
        mixer[:, pl.ds(spot, lanes)] = (
            cot_in[:, pl.ds(block, lanes)].astype(f32) + gained[:, lanes * m : lanes * (m + 1)]
        ).astype(bf)
    mine = mixer.at[:, quarter(tp)]
    other = mixer.at[:, quarter(across)]
    last = [
        send(mine, mine, s_g.at[0], r_g.at[0], {"tp": across}),
        send(mine, mine, s_g.at[1], r_g.at[1], {"tp": mate}),
    ]

    is_hub = core == me % 2

    def toward(m):
        dest = 2 * m + core
        at = pl.ds(pl.multiple_of(tp * cols + m * lanes, lanes), lanes)
        copy = wire(mixer.at[:, at], all_mixer.at[row, me], s_m.at[m], r_m.at[me], {"sp": dest})
        return dest, at, copy

    for m in range(narrow):
        dest, at, copy = toward(m)

        @pl.when(dest != me)
        def _():
            copy.start()

        @pl.when(dest == me)
        def _():
            all_mixer[row, me] = mixer[:, at]

    for i in range(11, 11 + blocks):
        loads[i].wait()
    last[1].wait_recv()

    def heads_of(side):
        at = pl.ds(pl.multiple_of(side * 2 * cols, 2 * cols), 2 * cols)
        return dot(mixer[:, at], proj[at, :])

    raw = heads_of(row)
    last[0].wait_recv()
    last.append(send(other, other, s_g.at[2], r_g.at[2], {"tp": mate}))
    @pl.when(jnp.logical_not(inner))
    def _():
        landed(4)
        landed(6)

    lend(7, 4, 1).start()
    lend(8, 6, 1).start()
    for i in (5, 6, 7, 8):
        loads[i].wait()
    last[2].wait_recv()

    raw = raw + heads_of(1 - row)
    positions = (iota((tok, 2 * DK), 0)).astype(f32)
    lane = iota((tok, 2 * DK), 1)
    low = lane < DK
    all_heads = heads * narrow
    tokens = tok * experts
    scale = DK ** (-0.5)
    pairs = heads // 2
    cots, rate = [], []
    for p in range(pairs):
        ids = tp * heads + 2 * p + iota((1, 2 * DK), 1) // DK
        r = rates_of(ids, all_heads, tokens)
        rate.append(r)
        at = slice(2 * DK * p, 2 * DK * (p + 1))
        here = positions + (me * tok + 1).astype(f32)
        norm = jnp.sqrt((1.0 - jnp.exp(-2.0 * r)) / (1.0 - jnp.exp(-2.0 * r * here)))
        cot = (raw[:, at] * norm).astype(bf)
        cots.append(cot)
        lead = jnp.exp(-r * (positions + 1.0))
        lead_q = (query[:, at].astype(f32) * lead).astype(bf)
        both = dot(lead_q, cot, TN)
        state[DK * p : DK * (p + 1), :] = jnp.where(
            low[0:DK], both[0:DK, :], both[DK : 2 * DK, :]
        ).astype(bf)
    def hop(k):
        return wire(state, all_state.at[k // 2], s_b.at[k // 2], r_b.at[k // 2], {"sp": partner(me, k)})

    for k in HOPS:

        @pl.when(partner(me, k) < me)
        def _():
            hop(k).start()

    distance = (iota((tok, tok), 0) - iota((tok, tok), 1)).astype(f32)
    q_part, k_part, v_part = [], [], []
    zero = jnp.zeros((tok, 2 * DK), bf)
    shift = jnp.where(iota((DK, 2 * DK), 1) == iota((DK, 2 * DK), 0) + DK, 1.0, 0.0).astype(bf)
    keep = jnp.where(iota((DK, 2 * DK), 1) == iota((DK, 2 * DK), 0), 1.0, 0.0).astype(bf)
    for p in range(pairs):
        at = slice(2 * DK * p, 2 * DK * (p + 1))
        q, k_, v, cot = query[:, at], key[:, at], value[:, at], cots[p]
        gq = jnp.zeros((tok, 2 * DK), f32)
        gk = jnp.zeros((tok, 2 * DK), f32)
        gv = jnp.zeros((tok, 2 * DK), f32)
        for half in range(2):
            pick = low if half == 0 else jnp.logical_not(low)
            r = rates_of(tp * heads + 2 * p + half + iota((1, tok), 1) * 0, all_heads, tokens)
            down = jnp.where(distance >= 0, jnp.exp(-r * jnp.maximum(distance, 0.0)), 0.0)
            over = jnp.where(distance <= 0, jnp.exp(-r * jnp.maximum(-distance, 0.0)), 0.0)
            qh, kh = jnp.where(pick, q, zero), jnp.where(pick, k_, zero)
            vh, ch = jnp.where(pick, v, zero), jnp.where(pick, cot, zero)
            back_w = (dot(cot, vh, NT) * down).astype(bf)
            back_t = (dot(vh, cot, NT) * over).astype(bf)
            fwd_t = (dot(kh, q, NT) * scale * over).astype(bf)
            gq = gq + dot(back_w, kh)
            gk = gk + dot(back_t, qh)
            gv = gv + dot(fwd_t, ch)
        lead = jnp.exp(-rate[p] * (positions + 1.0))
        upper = dot(entry[2 * p].astype(bf), keep)
        lower = dot(entry[2 * p + 1].astype(bf), shift)
        held = jnp.concatenate([upper, lower], axis=0).astype(bf)
        gq = scale * gq + lead * dot(cot, held, NT)
        grad_q[:, at] = gq.astype(bf)
        k_part.append(gk)
        v_part.append(gv)

    def handover(i):
        held = all_mixer.at[row, i]
        return wire(held, held, s_h.at[0, i], r_h.at[0, i], {"tp": across})

    def handoff(half, i):
        held = all_mixer.at[half, i]
        return wire(held, held, s_h.at[1 + half, i], r_h.at[1 + half, i], {"tp": mate})

    def arrival(i):
        held = all_mixer.at[row, i]
        return wire(held, held, s_m.at[0], r_m.at[i], {"tp": mate})

    @pl.when(is_hub)
    def _():
        for k in (0,) + WAVE:
            i = partner(me, k)
            if k > 0:
                arrival(i).wait_recv()
            handover(i).start()
            handoff(row, i).start()

    for k in HOPS:

        @pl.when(partner(me, k) > me)
        def _():
            hop(k).wait_recv()

    def gathered(p, target):
        total = jnp.zeros((DK, 2 * DK), f32)
        for k in HOPS:
            ahead = partner(me, k) - target - 1
            reach = jnp.exp(-rate[p] * (jnp.maximum(ahead, 0) * tok).astype(f32))
            reach = reach * jnp.where(partner(me, k) > me, 1.0, 0.0)
            total = total + reach * all_state[k // 2, DK * p : DK * (p + 1), :].astype(f32)
        return total

    ahead_of_mate = jnp.where(me > xmate, 1.0, 0.0)
    for p in range(pairs):
        at = slice(DK * p, DK * (p + 1))
        given[at, :] = (gathered(p, xmate) + ahead_of_mate * state[at, :].astype(f32)).astype(bf)
    pass_on = send(given, all_state.at[0], s_b.at[0], r_b.at[0], {"sp": xmate})

    @pl.when(is_hub)
    def _():
        for k in (0,) + WAVE:
            i = partner(me, k)
            handover(i).wait_recv()
            handoff(1 - row, i).start()

    @pl.when(jnp.logical_not(is_hub))
    def _():
        for half in range(2):
            for i in range(experts):
                handoff(half, i).wait_recv()

    for block in (1, 3, 5, 7):
        landed(block)
    for half in range(2):
        at = slice(half * (pcols // 2), (half + 1) * (pcols // 2))
        grad_proj[at, :] = dot(
            all_mixer[half].reshape(experts * tok, pcols // 2),
            all_out[...].reshape(experts * tok, all_out.shape[2]),
            TN,
        )
    pass_on.wait_recv()
    for p in range(pairs):
        at = slice(2 * DK * p, 2 * DK * (p + 1))
        later = gathered(p, me) + all_state[0, DK * p : DK * (p + 1), :].astype(f32)
        whole = jnp.concatenate(
            [jnp.where(low[0:DK], later, 0.0), jnp.where(low[0:DK], 0.0, later)], axis=0
        ).astype(bf)
        tail = jnp.exp(-rate[p] * (tok - 1.0 - positions))
        grad_k[:, at] = (scale * (k_part[p] + tail * dot(value[:, at], whole, NT))).astype(bf)
        grad_v[:, at] = (v_part[p] + scale * tail * dot(key[:, at], whole)).astype(bf)

    for group in (far, side, near, relayed, parted, crossed, gone):
        for copy in group.values():
            copy.wait_send()
    for copy in last:
        copy.wait_send()
    pass_on.wait_send()
    for slot, block, step in ((0, 0, 2), (1, 0, 1), (2, 2, 1), (7, 4, 1), (8, 6, 1)):
        lend(slot, block, step).wait_send()

    @pl.when(inner)
    def _():
        for slot, block, step in ((3, 0, 6), (4, 2, 6), (5, 6, 2), (6, 4, 2)):
            lend(slot, block, step).wait_send()

    for k in HOPS:

        @pl.when(partner(me, k) < me)
        def _():
            hop(k).wait_send()

    for m in range(narrow):
        dest, at, copy = toward(m)

        @pl.when(dest != me)
        def _():
            copy.wait_send()

    @pl.when(is_hub)
    def _():
        for i in range(experts):
            handover(i).wait_send()
            handoff(0, i).wait_send()
            handoff(1, i).wait_send()


def settle_kernel(count, *refs):
    sources, targets, done = refs[:count], refs[count : 2 * count], refs[2 * count]
    copies = []
    for i in range(count):
        target = targets[i]
        if len(target.shape) > len(sources[i].shape):
            target = target.at[0]
        copies.append(pltpu.make_async_copy(sources[i], target, done.at[i]))
    for copy in copies:
        copy.start()
    for copy in copies:
        copy.wait()


def settle(arrays, shapes):
    count = len(arrays)
    return pl.pallas_call(
        functools.partial(settle_kernel, count),
        out_shape=tuple(jax.ShapeDtypeStruct(s, a.dtype) for s, a in zip(shapes, arrays)),
        in_specs=[pl.BlockSpec(memory_space=pl.ANY)] * count,
        out_specs=(pl.BlockSpec(memory_space=pl.ANY),) * count,
        scratch_shapes=[pltpu.SemaphoreType.DMA((count,))],
        compiler_params=pltpu.CompilerParams(vmem_limit_bytes=1024 * 1024),
    )(*arrays)


def mega(routes, gains, rows, cot, gate, up, down, proj, query, key, value, out, entry, experts, narrow):
    tok, width = rows.shape
    top = routes.shape[0]
    cap = 2 * tok * top // experts
    share = cap // narrow
    hidden = gate.shape[2]
    hv = query.shape[1]
    cols, pcols = width // narrow, width // experts
    heads = hv // DK
    bf, f32 = jnp.bfloat16, jnp.float32
    sem = pltpu.SemaphoreType.DMA
    any_spec = pl.BlockSpec(memory_space=pl.ANY)
    n = experts
    v = pltpu.VMEM
    results = pl.pallas_call(
        functools.partial(mega_kernel, experts, narrow),
        out_shape=(
            v(gate.shape[1:], bf),
            v(up.shape[1:], bf),
            v(down.shape[1:], bf),
            v((pcols, hv), f32),
            v(query.shape, bf),
            v(query.shape, bf),
            v(query.shape, bf),
        ),
        in_specs=[VMEM] * 2 + [pl.BlockSpec(memory_space=pltpu.HBM)] * 11,
        out_specs=(VMEM,) * 7,
        scratch_shapes=[
            v((tok, width), bf),
            v((tok, width), bf),
            v((width, hidden), bf),
            v((width, hidden), bf),
            v((hidden, width), bf),
            v((hidden, width), bf),
            v((hidden, width), bf),
            v((width, hidden), bf),
            v((width, hv), bf),
            v((tok, hv), bf),
            v((tok, hv), bf),
            v((tok, hv), bf),
            v((heads, DK, DK), f32),
            v((n * share, width), bf),
            v((n * share, width), bf),
            v((2, share, width), bf),
            v((n * cap, width), bf),
            v((n * cap, width), bf),
            v((tok, tok), f32),
            v((tok, tok), f32),
            v((n * cap, hidden), bf),
            v((n * cap, hidden), bf),
            v((n * cap, hidden), bf),
            v((n * cap, width), bf),
            v((n, 2, cap, cols), bf),
            v((n, cap, cols), bf),
            v((n, cap, cols), bf),
            v((n, cap, cols), bf),
            v((n, cap, cols), bf),
            v((tok, width), bf),
            v((n, tok, hv), bf),
            v((2, n, tok, pcols // 2), bf),
            v((heads // 2 * DK, 2 * DK), bf),
            v((heads // 2 * DK, 2 * DK), bf),
            v((n // 2, heads // 2 * DK, 2 * DK), bf),
            sem((11 + width // 128,)),
            sem((2, n)), sem((2, n)), sem((2, n)), sem((2, n)), sem((2, 2, n)), sem((2, 2, n)),
            sem((n, 2)), sem((n, 2)), sem((n,)), sem((n,)), sem((n,)), sem((n,)), sem((3,)), sem((3,)),
            sem((9,)), sem((n,)), sem((narrow,)), sem((n,)), sem((3, n)), sem((3, n)), sem((n // 2,)), sem((n // 2,)),
        ],
        compiler_params=pltpu.CompilerParams(
            collective_id=0, has_side_effects=True, vmem_limit_bytes=62800000
        ),
    )(routes, gains, rows, cot, gate, up, down, proj, query, key, value, out, entry)
    flat = (tok, hv)
    return settle(results, (gate.shape, up.shape, down.shape, (pcols, hv), flat, flat, flat))


def decay_rates(head_ids, head_count, token_count):
    half_count = head_count // 2
    fraction = jnp.minimum(head_ids, half_count) / half_count
    base_rate = jnp.exp(
        (1.0 - fraction) * jnp.log(1.0 / 32.0) + fraction * jnp.log(1.0 / token_count)
    )
    return base_rate * (1.0 + jnp.maximum(head_ids - half_count, 0.0) / half_count)


def position_norm(positions, head_rates):
    return jnp.sqrt(
        jnp.expm1(-2.0 * head_rates)[None, :]
        / jnp.expm1(-2.0 * head_rates[None, :] * (positions[:, None] + 1.0))
    )


def expert_grads(exp_rows, exp_cot, activated, d_gate, d_up):
    row_dims = (((0,), (0,)), ((), ()))
    grad_gate = lax.dot_general(
        exp_rows, d_gate, row_dims, preferred_element_type=jnp.float32
    ).astype(jnp.bfloat16)
    grad_up = lax.dot_general(exp_rows, d_up, row_dims, preferred_element_type=jnp.float32).astype(
        jnp.bfloat16
    )
    grad_down = lax.dot_general(
        activated, exp_cot, row_dims, preferred_element_type=jnp.float32
    ).astype(jnp.bfloat16)
    return (grad_gate[None], grad_up[None], grad_down[None])


def per_device(
    layer_input,
    out_cot,
    routes,
    route_weights,
    gate_weights,
    up_weights,
    down_weights,
    out_proj,
    queries,
    keys,
    values,
    mixer_out,
    entry_states,
):
    tok_rows, model_width = layer_input.shape
    experts = lax.axis_size("sp")
    narrow = lax.axis_size("tp")
    top_count = routes.shape[1]
    hidden, hv = gate_weights.shape[2], queries.shape[1]
    fits = top_count == 2 and tok_rows == SPAN and narrow == 4 and experts == 8
    fits = fits and 2 * tok_rows * top_count == experts * 64 and hidden % 128 == 0
    if fits and model_width % (experts * 256) == 0 and hv % 128 == 0:
        return mega(
            routes.T,
            route_weights.T,
            layer_input,
            out_cot,
            gate_weights,
            up_weights,
            down_weights,
            out_proj,
            queries,
            keys,
            values,
            mixer_out,
            entry_states,
            experts,
            narrow,
        )
    pair_count = tok_rows * top_count
    capacity = 2 * pair_count // experts
    flat_routes = routes.reshape(pair_count)
    onehot = (flat_routes[:, None] == jnp.arange(experts, dtype=jnp.int32)[None, :]).astype(
        jnp.int32
    )
    earlier = jnp.cumsum(onehot, axis=0) - onehot
    target = flat_routes * capacity + jnp.sum(earlier * onehot, axis=1)
    share = capacity // narrow
    first_row = lax.axis_index("tp") * share
    owner_tok = jnp.arange(pair_count, dtype=jnp.int32) // top_count
    slot_tok = jnp.full((experts * capacity,), tok_rows, jnp.int32).at[target].set(owner_tok)
    slot_weight = (
        jnp.zeros((experts * capacity,), jnp.float32)
        .at[target]
        .set(route_weights.reshape(pair_count))
    )
    blank_row = jnp.zeros((1, model_width), jnp.bfloat16)
    sent_rows = jnp.concatenate([layer_input, blank_row], 0)[slot_tok].reshape(
        experts, capacity, model_width
    )
    picked_cot = jnp.concatenate([out_cot, blank_row], 0)[slot_tok]
    sent_cot = (
        (slot_weight[:, None] * picked_cot.astype(jnp.float32))
        .astype(jnp.bfloat16)
        .reshape(experts, capacity, model_width)
    )
    part_rows = lax.dynamic_slice_in_dim(sent_rows, first_row, share, 1)
    part_cot = lax.dynamic_slice_in_dim(sent_cot, first_row, share, 1)
    got_rows, got_cot = (
        lax.all_to_all(part_rows, "sp", split_axis=0, concat_axis=0, tiled=True),
        lax.all_to_all(part_cot, "sp", split_axis=0, concat_axis=0, tiled=True),
    )
    got_rows, got_cot = (
        lax.all_gather(got_rows, "tp", axis=1, tiled=True),
        lax.all_gather(got_cot, "tp", axis=1, tiled=True),
    )
    exp_rows = got_rows.reshape(experts * capacity, model_width)
    exp_cot = got_cot.reshape(experts * capacity, model_width)
    gate_w = gate_weights[0]
    up_w = up_weights[0]
    down_w = down_weights[0]
    gate_pre = jnp.dot(exp_rows, gate_w, preferred_element_type=jnp.float32)
    up_pre = jnp.dot(exp_rows, up_w, preferred_element_type=jnp.float32)
    sigmoid_g = jax.nn.sigmoid(gate_pre)
    activated = (gate_pre * sigmoid_g * up_pre).astype(jnp.bfloat16)
    width_dims = (((1,), (1,)), ((), ()))
    d_act = lax.dot_general(exp_cot, down_w, width_dims, preferred_element_type=jnp.float32)
    d_gate = (d_act * up_pre * sigmoid_g * (1.0 + gate_pre * (1.0 - sigmoid_g))).astype(
        jnp.bfloat16
    )
    d_up = (d_act * gate_pre * sigmoid_g).astype(jnp.bfloat16)
    grads = expert_grads(exp_rows, exp_cot, activated, d_gate, d_up)
    partial_sum = lax.dot_general(d_gate, gate_w, width_dims, preferred_element_type=jnp.float32)
    partial_sum = partial_sum + lax.dot_general(
        d_up, up_w, width_dims, preferred_element_type=jnp.float32
    )
    summed = lax.psum_scatter(
        partial_sum.reshape(experts, capacity, model_width), "tp", scatter_dimension=2, tiled=True
    )
    returned = lax.all_to_all(
        summed.astype(jnp.bfloat16), "sp", split_axis=0, concat_axis=0, tiled=True
    )
    col_count = model_width // narrow
    first_col = lax.axis_index("tp") * col_count
    back_flat = returned.reshape(experts * capacity, col_count)
    pair_back = back_flat[target].reshape(tok_rows, top_count, col_count).astype(jnp.float32)
    own_cols = lax.dynamic_slice_in_dim(out_cot, first_col, col_count, 1).astype(jnp.float32)
    cot_cols = (own_cols + jnp.sum(pair_back, axis=1)).astype(jnp.bfloat16)
    mixer_cot = lax.all_gather(cot_cols, "tp", axis=1, tiled=True)
    head_count = queries.shape[1] // DK
    head_ids = (lax.axis_index("tp") * head_count + jnp.arange(head_count, dtype=jnp.int32)).astype(
        jnp.float32
    )
    head_rates = decay_rates(head_ids, head_count * narrow, tok_rows * experts)
    positions = (lax.axis_index("sp") * tok_rows + jnp.arange(tok_rows, dtype=jnp.int32)).astype(
        jnp.float32
    )
    head_cot = jnp.dot(mixer_cot, out_proj, preferred_element_type=jnp.float32).reshape(
        tok_rows, head_count, DK
    )
    head_cot = (head_cot * position_norm(positions, head_rates)[:, :, None]).astype(jnp.bfloat16)
    span_count = tok_rows // SPAN
    span_shape = (span_count, SPAN, head_count, DK)
    span_query = queries.reshape(span_shape)
    span_key = keys.reshape(span_shape)
    span_value = values.reshape(span_shape)
    span_cot = head_cot.reshape(span_shape)
    key_scale = DK ** (-0.5)
    offsets = jnp.arange(SPAN, dtype=jnp.float32)
    distance = offsets[:, None] - offsets[None, :]
    decay_mat = jnp.where(
        distance[None] >= 0,
        jnp.exp(-head_rates[:, None, None] * jnp.maximum(distance, 0.0)[None]),
        0.0,
    )
    fwd_weights = (
        jnp.einsum("cihd,cjhd->chij", span_query, span_key, preferred_element_type=jnp.float32)
        * key_scale
        * decay_mat[None]
    ).astype(jnp.bfloat16)
    back_weights = (
        jnp.einsum("cihd,cjhd->chij", span_cot, span_value, preferred_element_type=jnp.float32)
        * decay_mat[None]
    ).astype(jnp.bfloat16)
    tail_decay = jnp.exp(-head_rates[None, :] * (SPAN - 1.0 - offsets)[:, None])
    lead_decay = jnp.exp(-head_rates[None, :] * (offsets + 1.0)[:, None])
    query_wide = span_query.astype(jnp.float32)
    key_wide = span_key.astype(jnp.float32)
    value_wide = span_value.astype(jnp.float32)
    cot_wide = span_cot.astype(jnp.float32)
    backs = jnp.einsum(
        "cihd,cihe->chde",
        query_wide * lead_decay[None, :, :, None],
        cot_wide,
        precision=lax.Precision.HIGHEST,
    )
    own_back = backs[0]
    ahead = jnp.arange(experts, dtype=jnp.int32) - lax.axis_index("sp") - 1
    reach = jnp.where(
        ahead[:, None] >= 0,
        jnp.exp(-head_rates[None, :] * (jnp.maximum(ahead, 0) * tok_rows)[:, None]),
        0.0,
    )
    all_backs = lax.all_gather(own_back, "sp")
    rev_states = jnp.sum(reach[:, :, None, None] * all_backs, axis=0)[None]
    grad_proj = lax.psum_scatter(
        lax.dot_general(
            mixer_cot, mixer_out, (((0,), (0,)), ((), ())), preferred_element_type=jnp.float32
        ),
        "sp",
        scatter_dimension=0,
        tiled=True,
    )
    fwd_stack = entry_states
    grad_q = key_scale * jnp.einsum(
        "chij,cjhd->cihd", back_weights, span_key, preferred_element_type=jnp.float32
    )
    grad_q = grad_q + lead_decay[None, :, :, None] * jnp.einsum(
        "chde,cihe->cihd", fwd_stack, cot_wide, precision=lax.Precision.HIGHEST
    )
    grad_k = jnp.einsum(
        "chij,cihd->cjhd", back_weights, span_query, preferred_element_type=jnp.float32
    )
    grad_k = key_scale * (
        grad_k
        + tail_decay[None, :, :, None]
        * jnp.einsum("chde,cjhe->cjhd", rev_states, value_wide, precision=lax.Precision.HIGHEST)
    )
    grad_v = jnp.einsum(
        "chij,cihe->cjhe", fwd_weights, span_cot, preferred_element_type=jnp.float32
    )
    grad_v = grad_v + key_scale * tail_decay[None, :, :, None] * jnp.einsum(
        "chde,cjhd->cjhe", rev_states, key_wide, precision=lax.Precision.HIGHEST
    )
    flat_shape = (tok_rows, head_count * DK)
    return (
        grads[0],
        grads[1],
        grads[2],
        grad_proj,
        grad_q.reshape(flat_shape).astype(jnp.bfloat16),
        grad_k.reshape(flat_shape).astype(jnp.bfloat16),
        grad_v.reshape(flat_shape).astype(jnp.bfloat16),
    )


def solution(mesh):
    placed = (
        P("sp", None),
        P("sp", None),
        P("sp", None),
        P("sp", None),
        P("sp", None, "tp"),
        P("sp", None, "tp"),
        P("sp", "tp", None),
        P(None, "tp"),
        P("sp", "tp"),
        P("sp", "tp"),
        P("sp", "tp"),
        P("sp", "tp"),
        P("sp", "tp", None, None),
    )
    return jax.shard_map(
        per_device,
        mesh=mesh,
        in_specs=placed,
        out_specs=(
            P("sp", None, "tp"),
            P("sp", None, "tp"),
            P("sp", "tp", None),
            P("sp", "tp"),
            P("sp", "tp"),
            P("sp", "tp"),
            P("sp", "tp"),
        ),
        check_vma=False,
    )
```

```python
import functools
import math

import jax
import jax.numpy as jnp
from jax import lax
from jax.experimental import pallas as pl
from jax.experimental.pallas import tpu as pltpu
from jax.sharding import PartitionSpec as P

DK = 64
SPAN = 128
MESH = pl.DeviceIdType.MESH
VMEM = pl.BlockSpec(memory_space=pltpu.VMEM)


WAVE = (1, 4, 2, 5, 3, 6, 7)
HOPS = (2, 4, 6)
NT = (((1,), (1,)), ((), ()))
TN = (((0,), (0,)), ((), ()))


def partner(me, k):
    for bit in (1, 2, 4):
        if k & bit:
            me = me + bit - 2 * bit * ((me // bit) % 2)
    return me


def wire(src, dst, send_sem, recv_sem, target):
    return pltpu.make_async_remote_copy(
        src_ref=src,
        dst_ref=dst,
        send_sem=send_sem,
        recv_sem=recv_sem,
        device_id=target,
        device_id_type=MESH,
    )


def send(src, dst, send_sem, recv_sem, target):
    copy = wire(src, dst, send_sem, recv_sem, target)
    copy.start()
    return copy


def greet(experts, me, tp, narrow):
    barrier = pltpu.get_barrier_semaphore()
    for k in range(1, experts):
        pl.semaphore_signal(
            barrier, inc=1, device_id={"sp": (me + k) % experts}, device_id_type=MESH
        )
    for k in range(1, narrow):
        pl.semaphore_signal(
            barrier, inc=1, device_id={"tp": (tp + k) % narrow}, device_id_type=MESH
        )
    return barrier, experts + narrow - 2


def rates_of(ids, total, tokens):
    half = total // 2
    ids = ids.astype(jnp.float32)
    fraction = jnp.minimum(ids, float(half)) * (1.0 / half)
    low, high = math.log(1.0 / 32.0), math.log(1.0 / tokens)
    base = jnp.exp((1.0 - fraction) * low + fraction * high)
    return base * (1.0 + jnp.maximum(ids - float(half), 0.0) * (1.0 / half))


def iota(shape, dim):
    return lax.broadcasted_iota(jnp.int32, shape, dim)


def dot(a, b, dims=None):
    if dims is None:
        dims = (((1,), (0,)), ((), ()))
    return lax.dot_general(a, b, dims, preferred_element_type=jnp.float32)


def mega_kernel(
    experts,
    narrow,
    routes_hbm,
    gains_hbm,
    rows_hbm,
    cot_hbm,
    gate_hbm,
    up_hbm,
    down_hbm,
    proj_hbm,
    query_hbm,
    key_hbm,
    value_hbm,
    out_hbm,
    entry_hbm,
    gg,
    gu,
    gd,
    grad_proj,
    grad_q,
    grad_k,
    grad_v,
    routes,
    gains,
    rows_in,
    cot_in,
    gate_w,
    up_w,
    down_w,
    gate_t,
    up_t,
    down_t,
    proj,
    query,
    key,
    value,
    entry,
    rows_s,
    cot_s,
    extra,
    rbuf,
    cbuf,
    place,
    share_w,
    act,
    dg,
    du,
    part,
    near_buf,
    side_out,
    side_in,
    far_out,
    back,
    mixer,
    all_out,
    all_mixer,
    state,
    given,
    all_state,
    l_in,
    s_sp, r_sp, s_y, r_y, s_c, r_c,
    s_n, r_n, s_s, r_s, s_f, r_f, s_g, r_g,
    s_r, r_r, s_m, r_m, s_h, r_h, s_b, r_b,
):
    me, tp = lax.axis_index("sp"), lax.axis_index("tp")
    core, row = tp % 2, tp // 2
    mate, across = tp + 1 - 2 * core, (tp + 2) % narrow
    mate_core = 1 - core
    barrier, count = greet(experts, me, tp, narrow)
    tok, width = rows_in.shape
    share = rows_s.shape[0] // experts
    cap = share * narrow
    cols = width // narrow
    pcols = width // experts
    heads = query.shape[1] // DK
    bf = jnp.bfloat16
    f32 = jnp.float32
    xmate = partner(me, 1)

    loads = {}
    first_in = (
        (9, rows_hbm, rows_in),
        (10, cot_hbm, cot_in),
        (3, out_hbm, all_out.at[me]),
        (0, gate_hbm.at[0], gate_w),
        (1, up_hbm.at[0], up_w),
        (2, down_hbm.at[0], down_w),
        (5, query_hbm, query),
        (6, key_hbm, key),
        (7, value_hbm, value),
        (8, entry_hbm.at[0], entry),
    )
    lanes = 128
    width = rows_in.shape[1]
    blocks = width // lanes
    held_at = [
        (spot // narrow) // 2 + 2 * ((spot // narrow) % 2) + narrow * (spot % narrow)
        for spot in range(blocks)
    ]
    first_in = first_in + tuple(
        (
            11 + spot,
            proj_hbm.at[lanes * block : lanes * (block + 1)],
            proj.at[lanes * spot : lanes * (spot + 1)],
        )
        for spot, block in enumerate(held_at)
    )
    def fetch(some):
        for i, src, dst in some:
            loads[i] = pltpu.make_async_copy(src, dst, l_in.at[i])
            loads[i].start()

    tables = [
        pltpu.make_async_copy(src, dst, l_in.at[11 + blocks + i])
        for i, (src, dst) in enumerate(((routes_hbm, routes), (gains_hbm, gains)))
    ]
    for copy in tables:
        copy.start()
    fetch(first_in[:2])
    for copy in tables:
        copy.wait()

    named = iota((tok, tok), 0)
    first, second = routes[0:1, :] == named, routes[1:2, :] == named
    hit = jnp.logical_or(first, second)
    before = jnp.where(iota((tok, tok), 0) < iota((tok, tok), 1), 1.0, 0.0).astype(bf)
    rank = dot(jnp.where(hit, 1.0, 0.0).astype(bf), before)
    spot = jnp.where(hit, rank, -1.0)
    place[...] = spot
    gain = jnp.where(first, gains[0:1, :], 0.0) + jnp.where(second, gains[1:2, :], 0.0)
    share_w[...] = gain

    def spread_rows(a):
        return jnp.broadcast_to(
            a[0:experts][:, None, :], (experts, share, tok)
        ).reshape(experts * share, tok)

    slot = (iota((experts * share, tok), 0) % share + share * tp).astype(f32)
    mask = jnp.where(spread_rows(spot) == slot, 1.0, 0.0)
    part_gain = jnp.sum(mask * spread_rows(gain), axis=1, keepdims=True)
    chosen = mask.astype(bf)
    loads[9].wait()
    loads[10].wait()
    rows_s[...] = dot(chosen, rows_in[...]).astype(bf)
    cot_s[...] = (part_gain * dot(chosen, cot_in[...])).astype(bf)
    def piece(buf, origin, index):
        return buf.at[pl.ds(pl.multiple_of(origin * cap + index * share, share), share)]

    def block(buf, index):
        return buf.at[pl.ds(pl.multiple_of(index * share, share), share)]

    def hold(origin):
        return pl.ds(pl.multiple_of(origin * cap, cap), cap)

    def quarter(index):
        return pl.ds(pl.multiple_of(index * cols, cols), cols)

    fetch(first_in[2:6])
    pl.semaphore_wait(barrier, count)
    arrays = ((rows_s, rbuf), (cot_s, cbuf))
    inner = jnp.logical_or(me // 2 == 1, me // 2 == 2)

    def lend(slot, block, hop):
        index = block ^ hop
        held = all_out.at[partner(me, block)]
        return wire(held, held, s_r.at[slot], r_r.at[index], {"sp": partner(me, hop)})

    far, side, near, relayed = {}, {}, {}, {}
    for k in WAVE:
        peer = partner(me, k)
        for a, (src, dst) in enumerate(arrays):
            far[a, k] = send(
                block(src, peer), piece(dst, me, tp), s_sp.at[a, k], r_sp.at[a, k], {"sp": peer}
            )
        if k == 3:
            loads[3].wait()
            lend(0, 0, 2).start()
    near_slot = (iota((share, tok), 0) + share * across).astype(f32)
    near_mask = jnp.where(place[pl.ds(xmate, 1), :] == near_slot, 1.0, 0.0)
    near_gain = jnp.sum(near_mask * share_w[pl.ds(xmate, 1), :], axis=1, keepdims=True)
    near_chosen = near_mask.astype(bf)
    extra[0] = dot(near_chosen, rows_in[...]).astype(bf)
    extra[1] = (near_gain * dot(near_chosen, cot_in[...])).astype(bf)
    own_slot = iota((cap, tok), 0).astype(f32)
    own_mask = jnp.where(place[pl.ds(me, 1), :] == own_slot, 1.0, 0.0)
    own_gain = jnp.sum(own_mask * share_w[pl.ds(me, 1), :], axis=1, keepdims=True)
    own_chosen = own_mask.astype(bf)

    for a, (_, dst) in enumerate(arrays):
        side[a, 1] = send(
            extra.at[a], piece(dst, me, across), s_y.at[a, 1], r_y.at[a, 1], {"sp": xmate}
        )
    rbuf[hold(me), :] = dot(own_chosen, rows_in[...]).astype(bf)
    cbuf[hold(me), :] = (own_gain * dot(own_chosen, cot_in[...])).astype(bf)

    def landed(block):
        held = all_out.at[me]
        wire(held, held, s_r.at[0], r_r.at[block], {"sp": xmate}).wait_recv()


    def land(k):
        origin = partner(me, k)
        for a, (_, dst) in enumerate(arrays):
            far[a, k].wait_recv()
            held = piece(dst, origin, tp)
            if k > 1:
                side[a, k] = send(held, held, s_y.at[a, k], r_y.at[a, k], {"tp": across})
            near[a, k] = send(held, held, s_c.at[a, 0, k], r_c.at[a, 0, k], {"tp": mate})

    def relay(k):
        origin = partner(me, k)
        for a, (_, dst) in enumerate(arrays):
            side[a, k].wait_recv()
            held = piece(dst, origin, across)
            relayed[a, k] = send(held, held, s_c.at[a, 1, k], r_c.at[a, 1, k], {"tp": mate})

    def parting(k, half):
        return wire(
            part.at[hold(partner(me, k)), quarter(half * 2 + mate_core)],
            near_buf.at[k, half],
            s_n.at[k, half],
            r_n.at[k, half],
            {"tp": mate},
        )

    def chunk(ks):
        for k in ks:
            if k > 0:
                for a in range(2):
                    near[a, k].wait_recv()
                    relayed[a, k].wait_recv()
        size = len(ks) * cap
        at = pl.ds(pl.multiple_of(partner(me, ks[0]) // len(ks) * size, size), size)
        rows, cots = rbuf[at, :], cbuf[at, :]
        gate = dot(rows, gate_w[...])
        up = dot(rows, up_w[...])
        sig = jax.nn.sigmoid(gate)
        d_act = dot(cots, down_t[...])
        act[at, :] = (gate * sig * up).astype(bf)
        d_gate = (d_act * up * sig * (1.0 + gate * (1.0 - sig))).astype(bf)
        d_up = (d_act * gate * sig).astype(bf)
        dg[at, :] = d_gate
        du[at, :] = d_up
        sums = (dot(d_gate, gate_t[...]) + dot(d_up, up_t[...])).astype(bf)
        for spot, block in enumerate(held_at):
            part[at, lanes * spot : lanes * (spot + 1)] = sums[
                :, lanes * block : lanes * (block + 1)
            ]
        for k in ks:
            for half in range(2):
                parting(k, half).start()

    crossed, gone = {}, {}

    def cross(k):
        dest = partner(me, k)
        parting(k, 0).wait_recv()
        parting(k, 1).wait_recv()
        side_out[k] = (
            part[hold(dest), quarter(across)].astype(f32) + near_buf[k, 1 - row].astype(f32)
        ).astype(bf)
        crossed[k] = send(side_out.at[k], side_in.at[k], s_s.at[k], r_s.at[k], {"tp": across})

    def ship(k):
        dest = partner(me, k)
        crossed[k].wait_recv()
        done = (
            part[hold(dest), quarter(tp)].astype(f32)
            + near_buf[k, row].astype(f32)
            + side_in[k].astype(f32)
        ).astype(bf)
        if k == 0:
            back[me] = done
        else:
            far_out[k] = done
            gone[k] = send(far_out.at[k], back.at[me], s_f.at[k], r_f.at[k], {"sp": dest})

    def weight_grads(step):
        span = width // experts
        at = pl.ds(step * span, span)
        rows = rbuf[:, at]
        gg[at, :] = dot(rows, dg[...], TN).astype(bf)
        gu[at, :] = dot(rows, du[...], TN).astype(bf)
        gd[:, at] = dot(act[...], cbuf[:, at], TN).astype(bf)

    def early(when):
        @pl.when(when)
        def _():
            chunk((0, 1, 2, 3))

    def crossout():
        landed(2)
        lend(1, 0, 1).start()
        lend(2, 2, 1).start()

        @pl.when(inner)
        def _():
            lend(3, 0, 6).start()
            lend(4, 2, 6).start()

    def returnout():
        @pl.when(inner)
        def _():
            landed(6)
            landed(4)
            lend(3 + 2, 6, 2).start()
            lend(3 + 3, 4, 2).start()

    fetch(first_in[6:])
    turned = jnp.transpose(place[...])
    lane = iota((tok, 2 * cap), 1)
    picks = jnp.concatenate(
        [
            jnp.where(
                jnp.where(lane < cap, turned[:, 2 * p : 2 * p + 1], turned[:, 2 * p + 1 : 2 * p + 2])
                == (lane % cap).astype(f32),
                1.0,
                0.0,
            ).astype(bf)
            for p in range(experts // 2)
        ],
        axis=1,
    )
    for i in (0, 1, 2):
        loads[i].wait()
    for tile in range(experts):
        at = slice(tile * pcols, (tile + 1) * pcols)
        gate_t[:, at] = jnp.transpose(gate_w[at, :])
        up_t[:, at] = jnp.transpose(up_w[at, :])
        down_t[at, :] = jnp.transpose(down_w[:, at])
    land(1)
    land(4)
    land(2)
    relay(4)
    land(5)
    relay(2)
    land(3)
    relay(5)
    chunk((4, 5))
    relay(3)
    relay(1)
    cross(4)
    cross(5)
    chunk((0, 1, 2, 3))
    crossout()
    land(6)
    land(7)
    cross(2)
    cross(3)
    cross(1)
    cross(0)
    relay(6)
    ship(4)
    ship(5)
    relay(7)
    chunk((6, 7))
    ship(2)
    ship(3)
    cross(6)
    cross(7)
    weight_grads(0)
    ship(1)
    weight_grads(1)
    ship(0)
    ship(6)
    ship(7)
    returnout()
    weight_grads(2)
    weight_grads(3)
    weight_grads(4)
    weight_grads(5)
    weight_grads(6)
    weight_grads(7)
    for k in WAVE:
        gone[k].wait_recv()
    slots = back[...].reshape(experts * cap, cols)
    gained = dot(picks, slots)
    for m in range(narrow):
        block = pl.multiple_of((narrow * m + 2 * core + row) * lanes, lanes)
        spot = pl.multiple_of(tp * cols + m * lanes, lanes)
        mixer[:, pl.ds(spot, lanes)] = (
            cot_in[:, pl.ds(block, lanes)].astype(f32) + gained[:, lanes * m : lanes * (m + 1)]
        ).astype(bf)
    mine = mixer.at[:, quarter(tp)]
    other = mixer.at[:, quarter(across)]
    last = [
        send(mine, mine, s_g.at[0], r_g.at[0], {"tp": across}),
        send(mine, mine, s_g.at[1], r_g.at[1], {"tp": mate}),
    ]

    is_hub = core == me % 2

    def toward(m):
        dest = 2 * m + core
        at = pl.ds(pl.multiple_of(tp * cols + m * lanes, lanes), lanes)
        copy = wire(mixer.at[:, at], all_mixer.at[row, me], s_m.at[m], r_m.at[me], {"sp": dest})
        return dest, at, copy

    for m in range(narrow):
        dest, at, copy = toward(m)

        @pl.when(dest != me)
        def _():
            copy.start()

        @pl.when(dest == me)
        def _():
            all_mixer[row, me] = mixer[:, at]

    for i in range(11, 11 + blocks):
        loads[i].wait()
    last[1].wait_recv()

    def heads_of(side):
        at = pl.ds(pl.multiple_of(side * 2 * cols, 2 * cols), 2 * cols)
        return dot(mixer[:, at], proj[at, :])

    def quarter_heads(index):
        return dot(mixer[:, quarter(index)], proj[quarter(index), :])

    raw = heads_of(row)
    last[0].wait_recv()
    last.append(send(other, other, s_g.at[2], r_g.at[2], {"tp": mate}))
    raw = raw + quarter_heads(across)
    for i in (5, 6, 7, 8):
        loads[i].wait()
    last[2].wait_recv()

    raw = raw + quarter_heads(narrow - 1 - tp)
    positions = (iota((tok, 2 * DK), 0)).astype(f32)
    lane = iota((tok, 2 * DK), 1)
    low = lane < DK
    all_heads = heads * narrow
    tokens = tok * experts
    scale = DK ** (-0.5)
    pairs = heads // 2
    cots, rate = [], []
    for p in range(pairs):
        ids = tp * heads + 2 * p + iota((1, 2 * DK), 1) // DK
        r = rates_of(ids, all_heads, tokens)
        rate.append(r)
        at = slice(2 * DK * p, 2 * DK * (p + 1))
        here = positions + (me * tok + 1).astype(f32)
        norm = jnp.sqrt((1.0 - jnp.exp(-2.0 * r)) / (1.0 - jnp.exp(-2.0 * r * here)))
        cot = (raw[:, at] * norm).astype(bf)
        cots.append(cot)
        lead = jnp.exp(-r * (positions + 1.0))
        lead_q = (query[:, at].astype(f32) * lead).astype(bf)
        both = dot(lead_q, cot, TN)
        state[DK * p : DK * (p + 1), :] = jnp.where(
            low[0:DK], both[0:DK, :], both[DK : 2 * DK, :]
        ).astype(bf)
    def hop(k):
        return wire(state, all_state.at[k // 2], s_b.at[k // 2], r_b.at[k // 2], {"sp": partner(me, k)})

    for k in HOPS:

        @pl.when(partner(me, k) < me)
        def _():
            hop(k).start()

    @pl.when(jnp.logical_not(inner))
    def _():
        landed(4)
        landed(6)

    lend(7, 4, 1).start()
    lend(8, 6, 1).start()
    distance = (iota((tok, tok), 0) - iota((tok, tok), 1)).astype(f32)
    q_part, k_part, v_part = [], [], []
    zero = jnp.zeros((tok, 2 * DK), bf)
    shift = jnp.where(iota((DK, 2 * DK), 1) == iota((DK, 2 * DK), 0) + DK, 1.0, 0.0).astype(bf)
    keep = jnp.where(iota((DK, 2 * DK), 1) == iota((DK, 2 * DK), 0), 1.0, 0.0).astype(bf)
    for p in range(pairs):
        at = slice(2 * DK * p, 2 * DK * (p + 1))
        q, k_, v, cot = query[:, at], key[:, at], value[:, at], cots[p]
        gq = jnp.zeros((tok, 2 * DK), f32)
        gk = jnp.zeros((tok, 2 * DK), f32)
        gv = jnp.zeros((tok, 2 * DK), f32)
        for half in range(2):
            pick = low if half == 0 else jnp.logical_not(low)
            r = rates_of(tp * heads + 2 * p + half + iota((1, tok), 1) * 0, all_heads, tokens)
            down = jnp.where(distance >= 0, jnp.exp(-r * jnp.maximum(distance, 0.0)), 0.0)
            over = jnp.where(distance <= 0, jnp.exp(-r * jnp.maximum(-distance, 0.0)), 0.0)
            qh, kh = jnp.where(pick, q, zero), jnp.where(pick, k_, zero)
            vh, ch = jnp.where(pick, v, zero), jnp.where(pick, cot, zero)
            back_w = (dot(cot, vh, NT) * down).astype(bf)
            back_t = (dot(vh, cot, NT) * over).astype(bf)
            fwd_t = (dot(kh, q, NT) * scale * over).astype(bf)
            gq = gq + dot(back_w, kh)
            gk = gk + dot(back_t, qh)
            gv = gv + dot(fwd_t, ch)
        lead = jnp.exp(-rate[p] * (positions + 1.0))
        upper = dot(entry[2 * p].astype(bf), keep)
        lower = dot(entry[2 * p + 1].astype(bf), shift)
        held = jnp.concatenate([upper, lower], axis=0).astype(bf)
        gq = scale * gq + lead * dot(cot, held, NT)
        grad_q[:, at] = gq.astype(bf)
        k_part.append(gk)
        v_part.append(gv)

    def handover(i):
        held = all_mixer.at[row, i]
        return wire(held, held, s_h.at[0, i], r_h.at[0, i], {"tp": across})

    def handoff(half, i):
        held = all_mixer.at[half, i]
        return wire(held, held, s_h.at[1 + half, i], r_h.at[1 + half, i], {"tp": mate})

    def arrival(i):
        held = all_mixer.at[row, i]
        return wire(held, held, s_m.at[0], r_m.at[i], {"tp": mate})

    @pl.when(is_hub)
    def _():
        for k in (0,) + WAVE:
            i = partner(me, k)
            if k > 0:
                arrival(i).wait_recv()
            handover(i).start()
            handoff(row, i).start()

    for k in HOPS:

        @pl.when(partner(me, k) > me)
        def _():
            hop(k).wait_recv()

    def gathered(p, target):
        total = jnp.zeros((DK, 2 * DK), f32)
        for k in HOPS:
            ahead = partner(me, k) - target - 1
            reach = jnp.exp(-rate[p] * (jnp.maximum(ahead, 0) * tok).astype(f32))
            held = all_state[k // 2, DK * p : DK * (p + 1), :].astype(f32)
            due = iota((DK, 2 * DK), 0) * 0 + partner(me, k) > me
            total = total + jnp.where(due, reach * held, 0.0)
        return total

    ahead_of_mate = jnp.where(me > xmate, 1.0, 0.0)
    for p in range(pairs):
        at = slice(DK * p, DK * (p + 1))
        given[at, :] = (gathered(p, xmate) + ahead_of_mate * state[at, :].astype(f32)).astype(bf)
    pass_on = send(given, all_state.at[0], s_b.at[0], r_b.at[0], {"sp": xmate})

    @pl.when(is_hub)
    def _():
        for k in (0,) + WAVE:
            i = partner(me, k)
            handover(i).wait_recv()
            handoff(1 - row, i).start()

    @pl.when(jnp.logical_not(is_hub))
    def _():
        for half in range(2):
            for i in range(experts):
                handoff(half, i).wait_recv()

    for block in (1, 3, 5, 7):
        landed(block)
    for half in range(2):
        at = slice(half * (pcols // 2), (half + 1) * (pcols // 2))
        grad_proj[at, :] = dot(
            all_mixer[half].reshape(experts * tok, pcols // 2),
            all_out[...].reshape(experts * tok, all_out.shape[2]),
            TN,
        )
    pass_on.wait_recv()
    for p in range(pairs):
        at = slice(2 * DK * p, 2 * DK * (p + 1))
        later = gathered(p, me) + all_state[0, DK * p : DK * (p + 1), :].astype(f32)
        whole = jnp.concatenate(
            [jnp.where(low[0:DK], later, 0.0), jnp.where(low[0:DK], 0.0, later)], axis=0
        ).astype(bf)
        tail = jnp.exp(-rate[p] * (tok - 1.0 - positions))
        grad_k[:, at] = (scale * (k_part[p] + tail * dot(value[:, at], whole, NT))).astype(bf)
        grad_v[:, at] = (v_part[p] + scale * tail * dot(key[:, at], whole)).astype(bf)

    for group in (far, side, near, relayed, crossed, gone):
        for copy in group.values():
            copy.wait_send()
    for k in range(experts):
        for half in range(2):
            parting(k, half).wait_send()
    for copy in last:
        copy.wait_send()
    pass_on.wait_send()
    for slot, block, step in ((0, 0, 2), (1, 0, 1), (2, 2, 1), (7, 4, 1), (8, 6, 1)):
        lend(slot, block, step).wait_send()

    @pl.when(inner)
    def _():
        for slot, block, step in ((3, 0, 6), (4, 2, 6), (5, 6, 2), (6, 4, 2)):
            lend(slot, block, step).wait_send()

    for k in HOPS:

        @pl.when(partner(me, k) < me)
        def _():
            hop(k).wait_send()

    for m in range(narrow):
        dest, at, copy = toward(m)

        @pl.when(dest != me)
        def _():
            copy.wait_send()

    @pl.when(is_hub)
    def _():
        for i in range(experts):
            handover(i).wait_send()
            handoff(0, i).wait_send()
            handoff(1, i).wait_send()


def settle_kernel(count, *refs):
    sources, targets, done = refs[:count], refs[count : 2 * count], refs[2 * count]
    copies = []
    for i in range(count):
        target = targets[i]
        if len(target.shape) > len(sources[i].shape):
            target = target.at[0]
        copies.append(pltpu.make_async_copy(sources[i], target, done.at[i]))
    for copy in copies:
        copy.start()
    for copy in copies:
        copy.wait()


def settle(arrays, shapes):
    count = len(arrays)
    return pl.pallas_call(
        functools.partial(settle_kernel, count),
        out_shape=tuple(jax.ShapeDtypeStruct(s, a.dtype) for s, a in zip(shapes, arrays)),
        in_specs=[pl.BlockSpec(memory_space=pl.ANY)] * count,
        out_specs=(pl.BlockSpec(memory_space=pl.ANY),) * count,
        scratch_shapes=[pltpu.SemaphoreType.DMA((count,))],
        compiler_params=pltpu.CompilerParams(vmem_limit_bytes=1024 * 1024),
    )(*arrays)


def mega(routes, gains, rows, cot, gate, up, down, proj, query, key, value, out, entry, experts, narrow):
    tok, width = rows.shape
    top = routes.shape[0]
    cap = 2 * tok * top // experts
    share = cap // narrow
    hidden = gate.shape[2]
    hv = query.shape[1]
    cols, pcols = width // narrow, width // experts
    heads = hv // DK
    bf, f32 = jnp.bfloat16, jnp.float32
    sem = pltpu.SemaphoreType.DMA
    any_spec = pl.BlockSpec(memory_space=pl.ANY)
    n = experts
    v = pltpu.VMEM
    results = pl.pallas_call(
        functools.partial(mega_kernel, experts, narrow),
        out_shape=(
            v(gate.shape[1:], bf),
            v(up.shape[1:], bf),
            v(down.shape[1:], bf),
            v((pcols, hv), f32),
            v(query.shape, bf),
            v(query.shape, bf),
            v(query.shape, bf),
        ),
        in_specs=[pl.BlockSpec(memory_space=pltpu.HBM)] * 13,
        out_specs=(VMEM,) * 7,
        scratch_shapes=[
            v(routes.shape, jnp.int32),
            v(gains.shape, f32),
            v((tok, width), bf),
            v((tok, width), bf),
            v((width, hidden), bf),
            v((width, hidden), bf),
            v((hidden, width), bf),
            v((hidden, width), bf),
            v((hidden, width), bf),
            v((width, hidden), bf),
            v((width, hv), bf),
            v((tok, hv), bf),
            v((tok, hv), bf),
            v((tok, hv), bf),
            v((heads, DK, DK), f32),
            v((n * share, width), bf),
            v((n * share, width), bf),
            v((2, share, width), bf),
            v((n * cap, width), bf),
            v((n * cap, width), bf),
            v((tok, tok), f32),
            v((tok, tok), f32),
            v((n * cap, hidden), bf),
            v((n * cap, hidden), bf),
            v((n * cap, hidden), bf),
            v((n * cap, width), bf),
            v((n, 2, cap, cols), bf),
            v((n, cap, cols), bf),
            v((n, cap, cols), bf),
            v((n, cap, cols), bf),
            v((n, cap, cols), bf),
            v((tok, width), bf),
            v((n, tok, hv), bf),
            v((2, n, tok, pcols // 2), bf),
            v((heads // 2 * DK, 2 * DK), bf),
            v((heads // 2 * DK, 2 * DK), bf),
            v((n // 2, heads // 2 * DK, 2 * DK), bf),
            sem((13 + width // 128,)),
            sem((2, n)), sem((2, n)), sem((2, n)), sem((2, n)), sem((2, 2, n)), sem((2, 2, n)),
            sem((n, 2)), sem((n, 2)), sem((n,)), sem((n,)), sem((n,)), sem((n,)), sem((3,)), sem((3,)),
            sem((9,)), sem((n,)), sem((narrow,)), sem((n,)), sem((3, n)), sem((3, n)), sem((n // 2,)), sem((n // 2,)),
        ],
        compiler_params=pltpu.CompilerParams(
            collective_id=0, has_side_effects=True, vmem_limit_bytes=62800000
        ),
    )(routes, gains, rows, cot, gate, up, down, proj, query, key, value, out, entry)
    flat = (tok, hv)
    return settle(results, (gate.shape, up.shape, down.shape, (pcols, hv), flat, flat, flat))


def decay_rates(head_ids, head_count, token_count):
    half_count = head_count // 2
    fraction = jnp.minimum(head_ids, half_count) / half_count
    base_rate = jnp.exp(
        (1.0 - fraction) * jnp.log(1.0 / 32.0) + fraction * jnp.log(1.0 / token_count)
    )
    return base_rate * (1.0 + jnp.maximum(head_ids - half_count, 0.0) / half_count)


def position_norm(positions, head_rates):
    return jnp.sqrt(
        jnp.expm1(-2.0 * head_rates)[None, :]
        / jnp.expm1(-2.0 * head_rates[None, :] * (positions[:, None] + 1.0))
    )


def expert_grads(exp_rows, exp_cot, activated, d_gate, d_up):
    row_dims = (((0,), (0,)), ((), ()))
    grad_gate = lax.dot_general(
        exp_rows, d_gate, row_dims, preferred_element_type=jnp.float32
    ).astype(jnp.bfloat16)
    grad_up = lax.dot_general(exp_rows, d_up, row_dims, preferred_element_type=jnp.float32).astype(
        jnp.bfloat16
    )
    grad_down = lax.dot_general(
        activated, exp_cot, row_dims, preferred_element_type=jnp.float32
    ).astype(jnp.bfloat16)
    return (grad_gate[None], grad_up[None], grad_down[None])


def per_device(
    layer_input,
    out_cot,
    routes,
    route_weights,
    gate_weights,
    up_weights,
    down_weights,
    out_proj,
    queries,
    keys,
    values,
    mixer_out,
    entry_states,
):
    tok_rows, model_width = layer_input.shape
    experts = lax.axis_size("sp")
    narrow = lax.axis_size("tp")
    top_count = routes.shape[1]
    hidden, hv = gate_weights.shape[2], queries.shape[1]
    fits = top_count == 2 and tok_rows == SPAN and narrow == 4 and experts == 8
    fits = fits and 2 * tok_rows * top_count == experts * 64 and hidden % 128 == 0
    if fits and model_width % (experts * 256) == 0 and hv % 128 == 0:
        return mega(
            routes.T,
            route_weights.T,
            layer_input,
            out_cot,
            gate_weights,
            up_weights,
            down_weights,
            out_proj,
            queries,
            keys,
            values,
            mixer_out,
            entry_states,
            experts,
            narrow,
        )
    pair_count = tok_rows * top_count
    capacity = 2 * pair_count // experts
    flat_routes = routes.reshape(pair_count)
    onehot = (flat_routes[:, None] == jnp.arange(experts, dtype=jnp.int32)[None, :]).astype(
        jnp.int32
    )
    earlier = jnp.cumsum(onehot, axis=0) - onehot
    target = flat_routes * capacity + jnp.sum(earlier * onehot, axis=1)
    share = capacity // narrow
    first_row = lax.axis_index("tp") * share
    owner_tok = jnp.arange(pair_count, dtype=jnp.int32) // top_count
    slot_tok = jnp.full((experts * capacity,), tok_rows, jnp.int32).at[target].set(owner_tok)
    slot_weight = (
        jnp.zeros((experts * capacity,), jnp.float32)
        .at[target]
        .set(route_weights.reshape(pair_count))
    )
    blank_row = jnp.zeros((1, model_width), jnp.bfloat16)
    sent_rows = jnp.concatenate([layer_input, blank_row], 0)[slot_tok].reshape(
        experts, capacity, model_width
    )
    picked_cot = jnp.concatenate([out_cot, blank_row], 0)[slot_tok]
    sent_cot = (
        (slot_weight[:, None] * picked_cot.astype(jnp.float32))
        .astype(jnp.bfloat16)
        .reshape(experts, capacity, model_width)
    )
    part_rows = lax.dynamic_slice_in_dim(sent_rows, first_row, share, 1)
    part_cot = lax.dynamic_slice_in_dim(sent_cot, first_row, share, 1)
    got_rows, got_cot = (
        lax.all_to_all(part_rows, "sp", split_axis=0, concat_axis=0, tiled=True),
        lax.all_to_all(part_cot, "sp", split_axis=0, concat_axis=0, tiled=True),
    )
    got_rows, got_cot = (
        lax.all_gather(got_rows, "tp", axis=1, tiled=True),
        lax.all_gather(got_cot, "tp", axis=1, tiled=True),
    )
    exp_rows = got_rows.reshape(experts * capacity, model_width)
    exp_cot = got_cot.reshape(experts * capacity, model_width)
    gate_w = gate_weights[0]
    up_w = up_weights[0]
    down_w = down_weights[0]
    gate_pre = jnp.dot(exp_rows, gate_w, preferred_element_type=jnp.float32)
    up_pre = jnp.dot(exp_rows, up_w, preferred_element_type=jnp.float32)
    sigmoid_g = jax.nn.sigmoid(gate_pre)
    activated = (gate_pre * sigmoid_g * up_pre).astype(jnp.bfloat16)
    width_dims = (((1,), (1,)), ((), ()))
    d_act = lax.dot_general(exp_cot, down_w, width_dims, preferred_element_type=jnp.float32)
    d_gate = (d_act * up_pre * sigmoid_g * (1.0 + gate_pre * (1.0 - sigmoid_g))).astype(
        jnp.bfloat16
    )
    d_up = (d_act * gate_pre * sigmoid_g).astype(jnp.bfloat16)
    grads = expert_grads(exp_rows, exp_cot, activated, d_gate, d_up)
    partial_sum = lax.dot_general(d_gate, gate_w, width_dims, preferred_element_type=jnp.float32)
    partial_sum = partial_sum + lax.dot_general(
        d_up, up_w, width_dims, preferred_element_type=jnp.float32
    )
    summed = lax.psum_scatter(
        partial_sum.reshape(experts, capacity, model_width), "tp", scatter_dimension=2, tiled=True
    )
    returned = lax.all_to_all(
        summed.astype(jnp.bfloat16), "sp", split_axis=0, concat_axis=0, tiled=True
    )
    col_count = model_width // narrow
    first_col = lax.axis_index("tp") * col_count
    back_flat = returned.reshape(experts * capacity, col_count)
    pair_back = back_flat[target].reshape(tok_rows, top_count, col_count).astype(jnp.float32)
    own_cols = lax.dynamic_slice_in_dim(out_cot, first_col, col_count, 1).astype(jnp.float32)
    cot_cols = (own_cols + jnp.sum(pair_back, axis=1)).astype(jnp.bfloat16)
    mixer_cot = lax.all_gather(cot_cols, "tp", axis=1, tiled=True)
    head_count = queries.shape[1] // DK
    head_ids = (lax.axis_index("tp") * head_count + jnp.arange(head_count, dtype=jnp.int32)).astype(
        jnp.float32
    )
    head_rates = decay_rates(head_ids, head_count * narrow, tok_rows * experts)
    positions = (lax.axis_index("sp") * tok_rows + jnp.arange(tok_rows, dtype=jnp.int32)).astype(
        jnp.float32
    )
    head_cot = jnp.dot(mixer_cot, out_proj, preferred_element_type=jnp.float32).reshape(
        tok_rows, head_count, DK
    )
    head_cot = (head_cot * position_norm(positions, head_rates)[:, :, None]).astype(jnp.bfloat16)
    span_count = tok_rows // SPAN
    span_shape = (span_count, SPAN, head_count, DK)
    span_query = queries.reshape(span_shape)
    span_key = keys.reshape(span_shape)
    span_value = values.reshape(span_shape)
    span_cot = head_cot.reshape(span_shape)
    key_scale = DK ** (-0.5)
    offsets = jnp.arange(SPAN, dtype=jnp.float32)
    distance = offsets[:, None] - offsets[None, :]
    decay_mat = jnp.where(
        distance[None] >= 0,
        jnp.exp(-head_rates[:, None, None] * jnp.maximum(distance, 0.0)[None]),
        0.0,
    )
    fwd_weights = (
        jnp.einsum("cihd,cjhd->chij", span_query, span_key, preferred_element_type=jnp.float32)
        * key_scale
        * decay_mat[None]
    ).astype(jnp.bfloat16)
    back_weights = (
        jnp.einsum("cihd,cjhd->chij", span_cot, span_value, preferred_element_type=jnp.float32)
        * decay_mat[None]
    ).astype(jnp.bfloat16)
    tail_decay = jnp.exp(-head_rates[None, :] * (SPAN - 1.0 - offsets)[:, None])
    lead_decay = jnp.exp(-head_rates[None, :] * (offsets + 1.0)[:, None])
    query_wide = span_query.astype(jnp.float32)
    key_wide = span_key.astype(jnp.float32)
    value_wide = span_value.astype(jnp.float32)
    cot_wide = span_cot.astype(jnp.float32)
    backs = jnp.einsum(
        "cihd,cihe->chde",
        query_wide * lead_decay[None, :, :, None],
        cot_wide,
        precision=lax.Precision.HIGHEST,
    )
    own_back = backs[0]
    ahead = jnp.arange(experts, dtype=jnp.int32) - lax.axis_index("sp") - 1
    reach = jnp.where(
        ahead[:, None] >= 0,
        jnp.exp(-head_rates[None, :] * (jnp.maximum(ahead, 0) * tok_rows)[:, None]),
        0.0,
    )
    all_backs = lax.all_gather(own_back, "sp")
    rev_states = jnp.sum(reach[:, :, None, None] * all_backs, axis=0)[None]
    grad_proj = lax.psum_scatter(
        lax.dot_general(
            mixer_cot, mixer_out, (((0,), (0,)), ((), ())), preferred_element_type=jnp.float32
        ),
        "sp",
        scatter_dimension=0,
        tiled=True,
    )
    fwd_stack = entry_states
    grad_q = key_scale * jnp.einsum(
        "chij,cjhd->cihd", back_weights, span_key, preferred_element_type=jnp.float32
    )
    grad_q = grad_q + lead_decay[None, :, :, None] * jnp.einsum(
        "chde,cihe->cihd", fwd_stack, cot_wide, precision=lax.Precision.HIGHEST
    )
    grad_k = jnp.einsum(
        "chij,cihd->cjhd", back_weights, span_query, preferred_element_type=jnp.float32
    )
    grad_k = key_scale * (
        grad_k
        + tail_decay[None, :, :, None]
        * jnp.einsum("chde,cjhe->cjhd", rev_states, value_wide, precision=lax.Precision.HIGHEST)
    )
    grad_v = jnp.einsum(
        "chij,cihe->cjhe", fwd_weights, span_cot, preferred_element_type=jnp.float32
    )
    grad_v = grad_v + key_scale * tail_decay[None, :, :, None] * jnp.einsum(
        "chde,cjhd->cjhe", rev_states, key_wide, precision=lax.Precision.HIGHEST
    )
    flat_shape = (tok_rows, head_count * DK)
    return (
        grads[0],
        grads[1],
        grads[2],
        grad_proj,
        grad_q.reshape(flat_shape).astype(jnp.bfloat16),
        grad_k.reshape(flat_shape).astype(jnp.bfloat16),
        grad_v.reshape(flat_shape).astype(jnp.bfloat16),
    )


def solution(mesh):
    placed = (
        P("sp", None),
        P("sp", None),
        P("sp", None),
        P("sp", None),
        P("sp", None, "tp"),
        P("sp", None, "tp"),
        P("sp", "tp", None),
        P(None, "tp"),
        P("sp", "tp"),
        P("sp", "tp"),
        P("sp", "tp"),
        P("sp", "tp"),
        P("sp", "tp", None, None),
    )
    return jax.shard_map(
        per_device,
        mesh=mesh,
        in_specs=placed,
        out_specs=(
            P("sp", None, "tp"),
            P("sp", None, "tp"),
            P("sp", "tp", None),
            P("sp", "tp"),
            P("sp", "tp"),
            P("sp", "tp"),
            P("sp", "tp"),
        ),
        check_vma=False,
    )
```

```python
import functools
import math

import jax
import jax.numpy as jnp
from jax import lax
from jax.experimental import pallas as pl
from jax.experimental.pallas import tpu as pltpu
from jax.sharding import PartitionSpec as P

DK = 64
SPAN = 128
MESH = pl.DeviceIdType.MESH
VMEM = pl.BlockSpec(memory_space=pltpu.VMEM)


WAVE = (1, 4, 2, 5, 3, 6, 7)
HOPS = (2, 4, 6)
SPLIT = (6, 7)
NT = (((1,), (1,)), ((), ()))
TN = (((0,), (0,)), ((), ()))


def partner(me, k):
    for bit in (1, 2, 4):
        if k & bit:
            me = me + bit - 2 * bit * ((me // bit) % 2)
    return me


def wire(src, dst, send_sem, recv_sem, target):
    return pltpu.make_async_remote_copy(
        src_ref=src,
        dst_ref=dst,
        send_sem=send_sem,
        recv_sem=recv_sem,
        device_id=target,
        device_id_type=MESH,
    )


def send(src, dst, send_sem, recv_sem, target):
    copy = wire(src, dst, send_sem, recv_sem, target)
    copy.start()
    return copy


def greet(experts, me, tp, narrow):
    barrier = pltpu.get_barrier_semaphore()
    for k in range(1, experts):
        pl.semaphore_signal(
            barrier, inc=1, device_id={"sp": (me + k) % experts}, device_id_type=MESH
        )
    for k in range(1, narrow):
        pl.semaphore_signal(
            barrier, inc=1, device_id={"tp": (tp + k) % narrow}, device_id_type=MESH
        )
    return barrier, experts + narrow - 2


def rates_of(ids, total, tokens):
    half = total // 2
    ids = ids.astype(jnp.float32)
    fraction = jnp.minimum(ids, float(half)) * (1.0 / half)
    low, high = math.log(1.0 / 32.0), math.log(1.0 / tokens)
    base = jnp.exp((1.0 - fraction) * low + fraction * high)
    return base * (1.0 + jnp.maximum(ids - float(half), 0.0) * (1.0 / half))


def iota(shape, dim):
    return lax.broadcasted_iota(jnp.int32, shape, dim)


def dot(a, b, dims=None):
    if dims is None:
        dims = (((1,), (0,)), ((), ()))
    return lax.dot_general(a, b, dims, preferred_element_type=jnp.float32)


def mega_kernel(
    experts,
    narrow,
    routes_hbm,
    gains_hbm,
    rows_hbm,
    cot_hbm,
    gate_hbm,
    up_hbm,
    down_hbm,
    proj_hbm,
    query_hbm,
    key_hbm,
    value_hbm,
    out_hbm,
    entry_hbm,
    gg,
    gu,
    gd,
    grad_proj,
    grad_q,
    grad_k,
    grad_v,
    routes,
    gains,
    rows_in,
    cot_in,
    gate_w,
    up_w,
    down_w,
    gate_t,
    up_t,
    down_t,
    proj,
    query,
    key,
    value,
    entry,
    rows_s,
    cot_s,
    extra,
    rbuf,
    cbuf,
    place,
    share_w,
    act,
    dg,
    du,
    part,
    near_buf,
    side_out,
    side_in,
    far_out,
    back,
    mixer,
    all_out,
    all_mixer,
    state,
    given,
    all_state,
    l_in,
    s_sp, r_sp, s_y, r_y, s_c, r_c,
    s_n, r_n, s_s, r_s, s_f, r_f, s_g, r_g,
    s_r, r_r, s_m, r_m, s_h, r_h, s_b, r_b,
):
    me, tp = lax.axis_index("sp"), lax.axis_index("tp")
    core, row = tp % 2, tp // 2
    mate, across = tp + 1 - 2 * core, (tp + 2) % narrow
    mate_core = 1 - core
    barrier, count = greet(experts, me, tp, narrow)
    tok, width = rows_in.shape
    share = rows_s.shape[0] // experts
    cap = share * narrow
    cols = width // narrow
    pcols = width // experts
    heads = query.shape[1] // DK
    bf = jnp.bfloat16
    f32 = jnp.float32
    xmate = partner(me, 1)

    loads = {}
    first_in = (
        (9, rows_hbm, rows_in),
        (10, cot_hbm, cot_in),
        (3, out_hbm, all_out.at[me]),
        (0, gate_hbm.at[0], gate_w),
        (1, up_hbm.at[0], up_w),
        (2, down_hbm.at[0], down_w),
        (5, query_hbm, query),
        (6, key_hbm, key),
        (7, value_hbm, value),
        (8, entry_hbm.at[0], entry),
    )
    lanes = 128
    width = rows_in.shape[1]
    blocks = width // lanes
    held_at = [
        (spot // narrow) // 2 + 2 * ((spot // narrow) % 2) + narrow * (spot % narrow)
        for spot in range(blocks)
    ]
    first_in = first_in + tuple(
        (
            11 + spot,
            proj_hbm.at[lanes * block : lanes * (block + 1)],
            proj.at[lanes * spot : lanes * (spot + 1)],
        )
        for spot, block in enumerate(held_at)
    )
    def fetch(some):
        for i, src, dst in some:
            loads[i] = pltpu.make_async_copy(src, dst, l_in.at[i])
            loads[i].start()

    tables = [
        pltpu.make_async_copy(src, dst, l_in.at[11 + blocks + i])
        for i, (src, dst) in enumerate(((routes_hbm, routes), (gains_hbm, gains)))
    ]
    for copy in tables:
        copy.start()
    fetch(first_in[:2])
    for copy in tables:
        copy.wait()

    named = iota((tok, tok), 0)
    first, second = routes[0:1, :] == named, routes[1:2, :] == named
    hit = jnp.logical_or(first, second)
    before = jnp.where(iota((tok, tok), 0) < iota((tok, tok), 1), 1.0, 0.0).astype(bf)
    rank = dot(jnp.where(hit, 1.0, 0.0).astype(bf), before)
    spot = jnp.where(hit, rank, -1.0)
    place[...] = spot
    gain = jnp.where(first, gains[0:1, :], 0.0) + jnp.where(second, gains[1:2, :], 0.0)
    share_w[...] = gain

    def spread_rows(a):
        return jnp.broadcast_to(
            a[0:experts][:, None, :], (experts, share, tok)
        ).reshape(experts * share, tok)

    slot = (iota((experts * share, tok), 0) % share + share * tp).astype(f32)
    mask = jnp.where(spread_rows(spot) == slot, 1.0, 0.0)
    part_gain = jnp.sum(mask * spread_rows(gain), axis=1, keepdims=True)
    chosen = mask.astype(bf)
    loads[9].wait()
    loads[10].wait()
    rows_s[...] = dot(chosen, rows_in[...]).astype(bf)
    cot_s[...] = (part_gain * dot(chosen, cot_in[...])).astype(bf)
    def piece(buf, origin, index):
        return buf.at[pl.ds(pl.multiple_of(origin * cap + index * share, share), share)]

    def block(buf, index):
        return buf.at[pl.ds(pl.multiple_of(index * share, share), share)]

    def hold(origin):
        return pl.ds(pl.multiple_of(origin * cap, cap), cap)

    def quarter(index):
        return pl.ds(pl.multiple_of(index * cols, cols), cols)

    fetch(first_in[2:6])
    pl.semaphore_wait(barrier, count)
    arrays = ((rows_s, rbuf), (cot_s, cbuf))
    inner = jnp.logical_or(me // 2 == 1, me // 2 == 2)

    def lend(slot, block, hop):
        index = block ^ hop
        held = all_out.at[partner(me, block)]
        return wire(held, held, s_r.at[slot], r_r.at[index], {"sp": partner(me, hop)})

    far, side, near, relayed = {}, {}, {}, {}
    for k in WAVE:
        peer = partner(me, k)
        for a, (src, dst) in enumerate(arrays):
            far[a, k] = send(
                block(src, peer), piece(dst, me, tp), s_sp.at[a, k], r_sp.at[a, k], {"sp": peer}
            )
        if k == 3:
            loads[3].wait()
            lend(0, 0, 2).start()
    near_slot = (iota((share, tok), 0) + share * across).astype(f32)
    near_mask = jnp.where(place[pl.ds(xmate, 1), :] == near_slot, 1.0, 0.0)
    near_gain = jnp.sum(near_mask * share_w[pl.ds(xmate, 1), :], axis=1, keepdims=True)
    near_chosen = near_mask.astype(bf)
    extra[0] = dot(near_chosen, rows_in[...]).astype(bf)
    extra[1] = (near_gain * dot(near_chosen, cot_in[...])).astype(bf)
    own_slot = iota((cap, tok), 0).astype(f32)
    own_mask = jnp.where(place[pl.ds(me, 1), :] == own_slot, 1.0, 0.0)
    own_gain = jnp.sum(own_mask * share_w[pl.ds(me, 1), :], axis=1, keepdims=True)
    own_chosen = own_mask.astype(bf)

    for a, (_, dst) in enumerate(arrays):
        side[a, 1] = send(
            extra.at[a], piece(dst, me, across), s_y.at[a, 1], r_y.at[a, 1], {"sp": xmate}
        )
    rbuf[hold(me), :] = dot(own_chosen, rows_in[...]).astype(bf)
    cbuf[hold(me), :] = (own_gain * dot(own_chosen, cot_in[...])).astype(bf)

    def landed(block):
        held = all_out.at[me]
        wire(held, held, s_r.at[0], r_r.at[block], {"sp": xmate}).wait_recv()


    def land(k):
        origin = partner(me, k)
        for a, (_, dst) in enumerate(arrays):
            far[a, k].wait_recv()
            held = piece(dst, origin, tp)
            if k > 1:
                side[a, k] = send(held, held, s_y.at[a, k], r_y.at[a, k], {"tp": across})
            near[a, k] = send(held, held, s_c.at[a, 0, k], r_c.at[a, 0, k], {"tp": mate})

    def relay(k):
        origin = partner(me, k)
        for a, (_, dst) in enumerate(arrays):
            side[a, k].wait_recv()
            held = piece(dst, origin, across)
            relayed[a, k] = send(held, held, s_c.at[a, 1, k], r_c.at[a, 1, k], {"tp": mate})

    def parting(k, half):
        return wire(
            part.at[hold(partner(me, k)), quarter(half * 2 + mate_core)],
            near_buf.at[k, half],
            s_n.at[k, half],
            r_n.at[k, half],
            {"tp": mate},
        )

    def chunk(ks):
        for k in ks:
            if k > 0:
                for a in range(2):
                    near[a, k].wait_recv()
                    relayed[a, k].wait_recv()
        size = len(ks) * cap
        at = pl.ds(pl.multiple_of(partner(me, ks[0]) // len(ks) * size, size), size)
        rows, cots = rbuf[at, :], cbuf[at, :]
        gate = dot(rows, gate_w[...])
        up = dot(rows, up_w[...])
        sig = jax.nn.sigmoid(gate)
        d_act = dot(cots, down_t[...])
        act[at, :] = (gate * sig * up).astype(bf)
        d_gate = (d_act * up * sig * (1.0 + gate * (1.0 - sig))).astype(bf)
        d_up = (d_act * gate * sig).astype(bf)
        dg[at, :] = d_gate
        du[at, :] = d_up
        sums = (dot(d_gate, gate_t[...]) + dot(d_up, up_t[...])).astype(bf)
        for spot, block in enumerate(held_at):
            part[at, lanes * spot : lanes * (spot + 1)] = sums[
                :, lanes * block : lanes * (block + 1)
            ]
        for k in ks:
            for half in range(2):
                parting(k, half).start()

    crossed, gone = {}, {}

    split = cols // 2
    sides = (0, 1)

    def halves(k):
        return sides if k in SPLIT else (None,)

    def span(half, base=None):
        start = 0 if half is None else half * split
        size = cols if half is None else split
        if base is None:
            return slice(start, start + size)
        return pl.ds(pl.multiple_of(base + start, size), size)

    def cross(k, half=None):
        dest = partner(me, k)
        index = half or 0
        if index == 0:
            parting(k, 0).wait_recv()
            parting(k, 1).wait_recv()
        at = span(half)
        side_out[k, :, at] = (
            part[hold(dest), span(half, across * cols)].astype(f32)
            + near_buf.at[k, 1 - row][:, at].astype(f32)
        ).astype(bf)
        crossed[k, half] = send(
            side_out.at[k, :, at],
            side_in.at[k, :, at],
            s_s.at[k, index],
            r_s.at[k, index],
            {"tp": across},
        )

    def ship(k, half=None):
        dest = partner(me, k)
        index = half or 0
        crossed[k, half].wait_recv()
        at = span(half)
        done = (
            part[hold(dest), span(half, tp * cols)].astype(f32)
            + near_buf.at[k, row][:, at].astype(f32)
            + side_in.at[k][:, at].astype(f32)
        ).astype(bf)
        if k == 0:
            back[me] = done
        else:
            far_out[k, :, at] = done
            gone[k, half] = send(
                far_out.at[k, :, at],
                back.at[me, :, at],
                s_f.at[k, index],
                r_f.at[k, index],
                {"sp": dest},
            )

    def weight_grads(step):
        span = width // experts
        at = pl.ds(step * span, span)
        rows = rbuf[:, at]
        gg[at, :] = dot(rows, dg[...], TN).astype(bf)
        gu[at, :] = dot(rows, du[...], TN).astype(bf)
        gd[:, at] = dot(act[...], cbuf[:, at], TN).astype(bf)

    def early(when):
        @pl.when(when)
        def _():
            chunk((0, 1, 2, 3))

    def crossout():
        landed(2)
        lend(1, 0, 1).start()
        lend(2, 2, 1).start()

        @pl.when(inner)
        def _():
            lend(3, 0, 6).start()
            lend(4, 2, 6).start()

    def returnout():
        @pl.when(inner)
        def _():
            landed(6)
            landed(4)
            lend(3 + 2, 6, 2).start()
            lend(3 + 3, 4, 2).start()

    fetch(first_in[6:])
    turned = jnp.transpose(place[...])
    lane = iota((tok, 2 * cap), 1)
    picks = jnp.concatenate(
        [
            jnp.where(
                jnp.where(lane < cap, turned[:, 2 * p : 2 * p + 1], turned[:, 2 * p + 1 : 2 * p + 2])
                == (lane % cap).astype(f32),
                1.0,
                0.0,
            ).astype(bf)
            for p in range(experts // 2)
        ],
        axis=1,
    )
    for i in (0, 1, 2):
        loads[i].wait()
    for tile in range(experts):
        at = slice(tile * pcols, (tile + 1) * pcols)
        gate_t[:, at] = jnp.transpose(gate_w[at, :])
        up_t[:, at] = jnp.transpose(up_w[at, :])
        down_t[at, :] = jnp.transpose(down_w[:, at])
    land(1)
    land(4)
    land(2)
    relay(4)
    land(5)
    relay(2)
    land(3)
    relay(5)
    chunk((4, 5))
    relay(3)
    relay(1)
    cross(4)
    cross(5)
    chunk((0, 1, 2, 3))
    land(6)
    land(7)
    cross(2)
    cross(3)
    cross(1)
    cross(0)
    ship(4)
    ship(5)
    crossout()
    relay(6)
    relay(7)
    chunk((6, 7))
    ship(2)
    ship(3)
    cross(6, 0)
    cross(7, 0)
    cross(6, 1)
    cross(7, 1)
    weight_grads(0)
    ship(1)
    weight_grads(1)
    ship(0)
    ship(6, 0)
    ship(7, 0)
    ship(6, 1)
    ship(7, 1)
    returnout()
    weight_grads(2)
    weight_grads(3)
    is_hub = core == me % 2

    def toward(m):
        dest = 2 * m + core
        at = pl.ds(pl.multiple_of(tp * cols + m * lanes, lanes), lanes)
        copy = wire(mixer.at[:, at], all_mixer.at[row, me], s_m.at[m], r_m.at[me], {"sp": dest})
        return dest, at, copy

    def strip(index, half):
        return mixer.at[:, span(half, index * cols)]

    def give(half, way):
        mine = strip(tp, half)
        return wire(mine, mine, s_g.at[half, way], r_g.at[half, way], {"tp": (across, mate)[way]})

    def regive(half):
        held = strip(across, half)
        return wire(held, held, s_g.at[half, 2], r_g.at[half, 2], {"tp": mate})

    for half in sides:
        for k in WAVE:
            if k in SPLIT:
                gone[k, half].wait_recv()
            elif half == 0:
                gone[k, None].wait_recv()
        slots = back[:, :, half * split : (half + 1) * split].reshape(experts * cap, split)
        gained = dot(picks, slots)
        for n in range(narrow // 2):
            m = half * (narrow // 2) + n
            block = pl.multiple_of((narrow * m + 2 * core + row) * lanes, lanes)
            spot = pl.multiple_of(tp * cols + m * lanes, lanes)
            mixer[:, pl.ds(spot, lanes)] = (
                cot_in[:, pl.ds(block, lanes)].astype(f32)
                + gained[:, lanes * n : lanes * (n + 1)]
            ).astype(bf)
        give(half, 0).start()
        give(half, 1).start()
        for n in range(narrow // 2):
            m = half * (narrow // 2) + n
            dest, at, copy = toward(m)

            @pl.when(dest != me)
            def _():
                copy.start()

            @pl.when(dest == me)
            def _():
                all_mixer[row, me] = mixer[:, at]

    for i in range(11, 11 + blocks):
        loads[i].wait()
    for half in sides:
        give(half, 1).wait_recv()

    def heads_of(side):
        at = pl.ds(pl.multiple_of(side * 2 * cols, 2 * cols), 2 * cols)
        return dot(mixer[:, at], proj[at, :])

    def quarter_heads(index):
        return dot(mixer[:, quarter(index)], proj[quarter(index), :])

    raw = heads_of(row)
    for half in sides:
        give(half, 0).wait_recv()
        regive(half).start()
    raw = raw + quarter_heads(across)
    for i in (5, 6, 7, 8):
        loads[i].wait()
    for half in sides:
        regive(half).wait_recv()

    raw = raw + quarter_heads(narrow - 1 - tp)
    positions = (iota((tok, 2 * DK), 0)).astype(f32)
    lane = iota((tok, 2 * DK), 1)
    low = lane < DK
    all_heads = heads * narrow
    tokens = tok * experts
    scale = DK ** (-0.5)
    pairs = heads // 2
    cots, rate = [], []
    for p in range(pairs):
        ids = tp * heads + 2 * p + iota((1, 2 * DK), 1) // DK
        r = rates_of(ids, all_heads, tokens)
        rate.append(r)
        at = slice(2 * DK * p, 2 * DK * (p + 1))
        here = positions + (me * tok + 1).astype(f32)
        norm = jnp.sqrt((1.0 - jnp.exp(-2.0 * r)) / (1.0 - jnp.exp(-2.0 * r * here)))
        cot = (raw[:, at] * norm).astype(bf)
        cots.append(cot)
        lead = jnp.exp(-r * (positions + 1.0))
        lead_q = (query[:, at].astype(f32) * lead).astype(bf)
        both = dot(lead_q, cot, TN)
        state[DK * p : DK * (p + 1), :] = jnp.where(
            low[0:DK], both[0:DK, :], both[DK : 2 * DK, :]
        ).astype(bf)
    def hop(k):
        return wire(state, all_state.at[k // 2], s_b.at[k // 2], r_b.at[k // 2], {"sp": partner(me, k)})

    for k in HOPS:

        @pl.when(partner(me, k) < me)
        def _():
            hop(k).start()

    @pl.when(jnp.logical_not(inner))
    def _():
        landed(4)
        landed(6)

    lend(7, 4, 1).start()
    lend(8, 6, 1).start()
    distance = (iota((tok, tok), 0) - iota((tok, tok), 1)).astype(f32)
    q_part, k_part, v_part = [], [], []
    zero = jnp.zeros((tok, 2 * DK), bf)
    shift = jnp.where(iota((DK, 2 * DK), 1) == iota((DK, 2 * DK), 0) + DK, 1.0, 0.0).astype(bf)
    keep = jnp.where(iota((DK, 2 * DK), 1) == iota((DK, 2 * DK), 0), 1.0, 0.0).astype(bf)
    for p in range(pairs):
        at = slice(2 * DK * p, 2 * DK * (p + 1))
        q, k_, v, cot = query[:, at], key[:, at], value[:, at], cots[p]
        gq = jnp.zeros((tok, 2 * DK), f32)
        gk = jnp.zeros((tok, 2 * DK), f32)
        gv = jnp.zeros((tok, 2 * DK), f32)
        for half in range(2):
            pick = low if half == 0 else jnp.logical_not(low)
            r = rates_of(tp * heads + 2 * p + half + iota((1, tok), 1) * 0, all_heads, tokens)
            down = jnp.where(distance >= 0, jnp.exp(-r * jnp.maximum(distance, 0.0)), 0.0)
            over = jnp.where(distance <= 0, jnp.exp(-r * jnp.maximum(-distance, 0.0)), 0.0)
            qh, kh = jnp.where(pick, q, zero), jnp.where(pick, k_, zero)
            vh, ch = jnp.where(pick, v, zero), jnp.where(pick, cot, zero)
            back_w = (dot(cot, vh, NT) * down).astype(bf)
            back_t = (dot(vh, cot, NT) * over).astype(bf)
            fwd_t = (dot(kh, q, NT) * scale * over).astype(bf)
            gq = gq + dot(back_w, kh)
            gk = gk + dot(back_t, qh)
            gv = gv + dot(fwd_t, ch)
        lead = jnp.exp(-rate[p] * (positions + 1.0))
        upper = dot(entry[2 * p].astype(bf), keep)
        lower = dot(entry[2 * p + 1].astype(bf), shift)
        held = jnp.concatenate([upper, lower], axis=0).astype(bf)
        gq = scale * gq + lead * dot(cot, held, NT)
        grad_q[:, at] = gq.astype(bf)
        k_part.append(gk)
        v_part.append(gv)

    def handover(i):
        held = all_mixer.at[row, i]
        return wire(held, held, s_h.at[0, i], r_h.at[0, i], {"tp": across})

    def handoff(half, i):
        held = all_mixer.at[half, i]
        return wire(held, held, s_h.at[1 + half, i], r_h.at[1 + half, i], {"tp": mate})

    def arrival(i):
        held = all_mixer.at[row, i]
        return wire(held, held, s_m.at[0], r_m.at[i], {"tp": mate})

    @pl.when(is_hub)
    def _():
        for k in (0,) + WAVE:
            i = partner(me, k)
            if k > 0:
                arrival(i).wait_recv()
            handover(i).start()
            handoff(row, i).start()

    weight_grads(4)
    weight_grads(5)
    weight_grads(6)
    weight_grads(7)
    for k in HOPS:

        @pl.when(partner(me, k) > me)
        def _():
            hop(k).wait_recv()

    def gathered(p, target):
        total = jnp.zeros((DK, 2 * DK), f32)
        for k in HOPS:
            ahead = partner(me, k) - target - 1
            reach = jnp.exp(-rate[p] * (jnp.maximum(ahead, 0) * tok).astype(f32))
            held = all_state[k // 2, DK * p : DK * (p + 1), :].astype(f32)
            due = iota((DK, 2 * DK), 0) * 0 + partner(me, k) > me
            total = total + jnp.where(due, reach * held, 0.0)
        return total

    ahead_of_mate = jnp.where(me > xmate, 1.0, 0.0)
    for p in range(pairs):
        at = slice(DK * p, DK * (p + 1))
        given[at, :] = (gathered(p, xmate) + ahead_of_mate * state[at, :].astype(f32)).astype(bf)
    pass_on = send(given, all_state.at[0], s_b.at[0], r_b.at[0], {"sp": xmate})

    @pl.when(is_hub)
    def _():
        for k in (0,) + WAVE:
            i = partner(me, k)
            handover(i).wait_recv()
            handoff(1 - row, i).start()

    @pl.when(jnp.logical_not(is_hub))
    def _():
        for half in range(2):
            for i in range(experts):
                handoff(half, i).wait_recv()

    for block in (1, 3, 5, 7):
        landed(block)
    for half in range(2):
        at = slice(half * (pcols // 2), (half + 1) * (pcols // 2))
        grad_proj[at, :] = dot(
            all_mixer[half].reshape(experts * tok, pcols // 2),
            all_out[...].reshape(experts * tok, all_out.shape[2]),
            TN,
        )
    pass_on.wait_recv()
    for p in range(pairs):
        at = slice(2 * DK * p, 2 * DK * (p + 1))
        later = gathered(p, me) + all_state[0, DK * p : DK * (p + 1), :].astype(f32)
        whole = jnp.concatenate(
            [jnp.where(low[0:DK], later, 0.0), jnp.where(low[0:DK], 0.0, later)], axis=0
        ).astype(bf)
        tail = jnp.exp(-rate[p] * (tok - 1.0 - positions))
        grad_k[:, at] = (scale * (k_part[p] + tail * dot(value[:, at], whole, NT))).astype(bf)
        grad_v[:, at] = (v_part[p] + scale * tail * dot(key[:, at], whole)).astype(bf)

    for group in (far, side, near, relayed, crossed, gone):
        for copy in group.values():
            copy.wait_send()
    for k in range(experts):
        for half in range(2):
            parting(k, half).wait_send()
    for half in sides:
        give(half, 0).wait_send()
        give(half, 1).wait_send()
        regive(half).wait_send()
    pass_on.wait_send()
    for slot, block, step in ((0, 0, 2), (1, 0, 1), (2, 2, 1), (7, 4, 1), (8, 6, 1)):
        lend(slot, block, step).wait_send()

    @pl.when(inner)
    def _():
        for slot, block, step in ((3, 0, 6), (4, 2, 6), (5, 6, 2), (6, 4, 2)):
            lend(slot, block, step).wait_send()

    for k in HOPS:

        @pl.when(partner(me, k) < me)
        def _():
            hop(k).wait_send()

    for m in range(narrow):
        dest, at, copy = toward(m)

        @pl.when(dest != me)
        def _():
            copy.wait_send()

    @pl.when(is_hub)
    def _():
        for i in range(experts):
            handover(i).wait_send()
            handoff(0, i).wait_send()
            handoff(1, i).wait_send()


def settle_kernel(count, *refs):
    sources, targets, done = refs[:count], refs[count : 2 * count], refs[2 * count]
    copies = []
    for i in range(count):
        target = targets[i]
        if len(target.shape) > len(sources[i].shape):
            target = target.at[0]
        copies.append(pltpu.make_async_copy(sources[i], target, done.at[i]))
    for copy in copies:
        copy.start()
    for copy in copies:
        copy.wait()


def settle(arrays, shapes):
    count = len(arrays)
    return pl.pallas_call(
        functools.partial(settle_kernel, count),
        out_shape=tuple(jax.ShapeDtypeStruct(s, a.dtype) for s, a in zip(shapes, arrays)),
        in_specs=[pl.BlockSpec(memory_space=pl.ANY)] * count,
        out_specs=(pl.BlockSpec(memory_space=pl.ANY),) * count,
        scratch_shapes=[pltpu.SemaphoreType.DMA((count,))],
        compiler_params=pltpu.CompilerParams(vmem_limit_bytes=1024 * 1024),
    )(*arrays)


def mega(routes, gains, rows, cot, gate, up, down, proj, query, key, value, out, entry, experts, narrow):
    tok, width = rows.shape
    top = routes.shape[0]
    cap = 2 * tok * top // experts
    share = cap // narrow
    hidden = gate.shape[2]
    hv = query.shape[1]
    cols, pcols = width // narrow, width // experts
    heads = hv // DK
    bf, f32 = jnp.bfloat16, jnp.float32
    sem = pltpu.SemaphoreType.DMA
    any_spec = pl.BlockSpec(memory_space=pl.ANY)
    n = experts
    v = pltpu.VMEM
    results = pl.pallas_call(
        functools.partial(mega_kernel, experts, narrow),
        out_shape=(
            v(gate.shape[1:], bf),
            v(up.shape[1:], bf),
            v(down.shape[1:], bf),
            v((pcols, hv), f32),
            v(query.shape, bf),
            v(query.shape, bf),
            v(query.shape, bf),
        ),
        in_specs=[pl.BlockSpec(memory_space=pltpu.HBM)] * 13,
        out_specs=(VMEM,) * 7,
        scratch_shapes=[
            v(routes.shape, jnp.int32),
            v(gains.shape, f32),
            v((tok, width), bf),
            v((tok, width), bf),
            v((width, hidden), bf),
            v((width, hidden), bf),
            v((hidden, width), bf),
            v((hidden, width), bf),
            v((hidden, width), bf),
            v((width, hidden), bf),
            v((width, hv), bf),
            v((tok, hv), bf),
            v((tok, hv), bf),
            v((tok, hv), bf),
            v((heads, DK, DK), f32),
            v((n * share, width), bf),
            v((n * share, width), bf),
            v((2, share, width), bf),
            v((n * cap, width), bf),
            v((n * cap, width), bf),
            v((tok, tok), f32),
            v((tok, tok), f32),
            v((n * cap, hidden), bf),
            v((n * cap, hidden), bf),
            v((n * cap, hidden), bf),
            v((n * cap, width), bf),
            v((n, 2, cap, cols), bf),
            v((n, cap, cols), bf),
            v((n, cap, cols), bf),
            v((n, cap, cols), bf),
            v((n, cap, cols), bf),
            v((tok, width), bf),
            v((n, tok, hv), bf),
            v((2, n, tok, pcols // 2), bf),
            v((heads // 2 * DK, 2 * DK), bf),
            v((heads // 2 * DK, 2 * DK), bf),
            v((n // 2, heads // 2 * DK, 2 * DK), bf),
            sem((13 + width // 128,)),
            sem((2, n)), sem((2, n)), sem((2, n)), sem((2, n)), sem((2, 2, n)), sem((2, 2, n)),
            sem((n, 2)), sem((n, 2)), sem((n, 2)), sem((n, 2)), sem((n, 2)), sem((n, 2)), sem((2, 3)), sem((2, 3)),
            sem((9,)), sem((n,)), sem((narrow,)), sem((n,)), sem((3, n)), sem((3, n)), sem((n // 2,)), sem((n // 2,)),
        ],
        compiler_params=pltpu.CompilerParams(
            collective_id=0, has_side_effects=True, vmem_limit_bytes=62800000
        ),
    )(routes, gains, rows, cot, gate, up, down, proj, query, key, value, out, entry)
    flat = (tok, hv)
    return settle(results, (gate.shape, up.shape, down.shape, (pcols, hv), flat, flat, flat))


def decay_rates(head_ids, head_count, token_count):
    half_count = head_count // 2
    fraction = jnp.minimum(head_ids, half_count) / half_count
    base_rate = jnp.exp(
        (1.0 - fraction) * jnp.log(1.0 / 32.0) + fraction * jnp.log(1.0 / token_count)
    )
    return base_rate * (1.0 + jnp.maximum(head_ids - half_count, 0.0) / half_count)


def position_norm(positions, head_rates):
    return jnp.sqrt(
        jnp.expm1(-2.0 * head_rates)[None, :]
        / jnp.expm1(-2.0 * head_rates[None, :] * (positions[:, None] + 1.0))
    )


def expert_grads(exp_rows, exp_cot, activated, d_gate, d_up):
    row_dims = (((0,), (0,)), ((), ()))
    grad_gate = lax.dot_general(
        exp_rows, d_gate, row_dims, preferred_element_type=jnp.float32
    ).astype(jnp.bfloat16)
    grad_up = lax.dot_general(exp_rows, d_up, row_dims, preferred_element_type=jnp.float32).astype(
        jnp.bfloat16
    )
    grad_down = lax.dot_general(
        activated, exp_cot, row_dims, preferred_element_type=jnp.float32
    ).astype(jnp.bfloat16)
    return (grad_gate[None], grad_up[None], grad_down[None])


def per_device(
    layer_input,
    out_cot,
    routes,
    route_weights,
    gate_weights,
    up_weights,
    down_weights,
    out_proj,
    queries,
    keys,
    values,
    mixer_out,
    entry_states,
):
    tok_rows, model_width = layer_input.shape
    experts = lax.axis_size("sp")
    narrow = lax.axis_size("tp")
    top_count = routes.shape[1]
    hidden, hv = gate_weights.shape[2], queries.shape[1]
    fits = top_count == 2 and tok_rows == SPAN and narrow == 4 and experts == 8
    fits = fits and 2 * tok_rows * top_count == experts * 64 and hidden % 128 == 0
    if fits and model_width % (experts * 256) == 0 and hv % 128 == 0:
        return mega(
            routes.T,
            route_weights.T,
            layer_input,
            out_cot,
            gate_weights,
            up_weights,
            down_weights,
            out_proj,
            queries,
            keys,
            values,
            mixer_out,
            entry_states,
            experts,
            narrow,
        )
    pair_count = tok_rows * top_count
    capacity = 2 * pair_count // experts
    flat_routes = routes.reshape(pair_count)
    onehot = (flat_routes[:, None] == jnp.arange(experts, dtype=jnp.int32)[None, :]).astype(
        jnp.int32
    )
    earlier = jnp.cumsum(onehot, axis=0) - onehot
    target = flat_routes * capacity + jnp.sum(earlier * onehot, axis=1)
    share = capacity // narrow
    first_row = lax.axis_index("tp") * share
    owner_tok = jnp.arange(pair_count, dtype=jnp.int32) // top_count
    slot_tok = jnp.full((experts * capacity,), tok_rows, jnp.int32).at[target].set(owner_tok)
    slot_weight = (
        jnp.zeros((experts * capacity,), jnp.float32)
        .at[target]
        .set(route_weights.reshape(pair_count))
    )
    blank_row = jnp.zeros((1, model_width), jnp.bfloat16)
    sent_rows = jnp.concatenate([layer_input, blank_row], 0)[slot_tok].reshape(
        experts, capacity, model_width
    )
    picked_cot = jnp.concatenate([out_cot, blank_row], 0)[slot_tok]
    sent_cot = (
        (slot_weight[:, None] * picked_cot.astype(jnp.float32))
        .astype(jnp.bfloat16)
        .reshape(experts, capacity, model_width)
    )
    part_rows = lax.dynamic_slice_in_dim(sent_rows, first_row, share, 1)
    part_cot = lax.dynamic_slice_in_dim(sent_cot, first_row, share, 1)
    got_rows, got_cot = (
        lax.all_to_all(part_rows, "sp", split_axis=0, concat_axis=0, tiled=True),
        lax.all_to_all(part_cot, "sp", split_axis=0, concat_axis=0, tiled=True),
    )
    got_rows, got_cot = (
        lax.all_gather(got_rows, "tp", axis=1, tiled=True),
        lax.all_gather(got_cot, "tp", axis=1, tiled=True),
    )
    exp_rows = got_rows.reshape(experts * capacity, model_width)
    exp_cot = got_cot.reshape(experts * capacity, model_width)
    gate_w = gate_weights[0]
    up_w = up_weights[0]
    down_w = down_weights[0]
    gate_pre = jnp.dot(exp_rows, gate_w, preferred_element_type=jnp.float32)
    up_pre = jnp.dot(exp_rows, up_w, preferred_element_type=jnp.float32)
    sigmoid_g = jax.nn.sigmoid(gate_pre)
    activated = (gate_pre * sigmoid_g * up_pre).astype(jnp.bfloat16)
    width_dims = (((1,), (1,)), ((), ()))
    d_act = lax.dot_general(exp_cot, down_w, width_dims, preferred_element_type=jnp.float32)
    d_gate = (d_act * up_pre * sigmoid_g * (1.0 + gate_pre * (1.0 - sigmoid_g))).astype(
        jnp.bfloat16
    )
    d_up = (d_act * gate_pre * sigmoid_g).astype(jnp.bfloat16)
    grads = expert_grads(exp_rows, exp_cot, activated, d_gate, d_up)
    partial_sum = lax.dot_general(d_gate, gate_w, width_dims, preferred_element_type=jnp.float32)
    partial_sum = partial_sum + lax.dot_general(
        d_up, up_w, width_dims, preferred_element_type=jnp.float32
    )
    summed = lax.psum_scatter(
        partial_sum.reshape(experts, capacity, model_width), "tp", scatter_dimension=2, tiled=True
    )
    returned = lax.all_to_all(
        summed.astype(jnp.bfloat16), "sp", split_axis=0, concat_axis=0, tiled=True
    )
    col_count = model_width // narrow
    first_col = lax.axis_index("tp") * col_count
    back_flat = returned.reshape(experts * capacity, col_count)
    pair_back = back_flat[target].reshape(tok_rows, top_count, col_count).astype(jnp.float32)
    own_cols = lax.dynamic_slice_in_dim(out_cot, first_col, col_count, 1).astype(jnp.float32)
    cot_cols = (own_cols + jnp.sum(pair_back, axis=1)).astype(jnp.bfloat16)
    mixer_cot = lax.all_gather(cot_cols, "tp", axis=1, tiled=True)
    head_count = queries.shape[1] // DK
    head_ids = (lax.axis_index("tp") * head_count + jnp.arange(head_count, dtype=jnp.int32)).astype(
        jnp.float32
    )
    head_rates = decay_rates(head_ids, head_count * narrow, tok_rows * experts)
    positions = (lax.axis_index("sp") * tok_rows + jnp.arange(tok_rows, dtype=jnp.int32)).astype(
        jnp.float32
    )
    head_cot = jnp.dot(mixer_cot, out_proj, preferred_element_type=jnp.float32).reshape(
        tok_rows, head_count, DK
    )
    head_cot = (head_cot * position_norm(positions, head_rates)[:, :, None]).astype(jnp.bfloat16)
    span_count = tok_rows // SPAN
    span_shape = (span_count, SPAN, head_count, DK)
    span_query = queries.reshape(span_shape)
    span_key = keys.reshape(span_shape)
    span_value = values.reshape(span_shape)
    span_cot = head_cot.reshape(span_shape)
    key_scale = DK ** (-0.5)
    offsets = jnp.arange(SPAN, dtype=jnp.float32)
    distance = offsets[:, None] - offsets[None, :]
    decay_mat = jnp.where(
        distance[None] >= 0,
        jnp.exp(-head_rates[:, None, None] * jnp.maximum(distance, 0.0)[None]),
        0.0,
    )
    fwd_weights = (
        jnp.einsum("cihd,cjhd->chij", span_query, span_key, preferred_element_type=jnp.float32)
        * key_scale
        * decay_mat[None]
    ).astype(jnp.bfloat16)
    back_weights = (
        jnp.einsum("cihd,cjhd->chij", span_cot, span_value, preferred_element_type=jnp.float32)
        * decay_mat[None]
    ).astype(jnp.bfloat16)
    tail_decay = jnp.exp(-head_rates[None, :] * (SPAN - 1.0 - offsets)[:, None])
    lead_decay = jnp.exp(-head_rates[None, :] * (offsets + 1.0)[:, None])
    query_wide = span_query.astype(jnp.float32)
    key_wide = span_key.astype(jnp.float32)
    value_wide = span_value.astype(jnp.float32)
    cot_wide = span_cot.astype(jnp.float32)
    backs = jnp.einsum(
        "cihd,cihe->chde",
        query_wide * lead_decay[None, :, :, None],
        cot_wide,
        precision=lax.Precision.HIGHEST,
    )
    own_back = backs[0]
    ahead = jnp.arange(experts, dtype=jnp.int32) - lax.axis_index("sp") - 1
    reach = jnp.where(
        ahead[:, None] >= 0,
        jnp.exp(-head_rates[None, :] * (jnp.maximum(ahead, 0) * tok_rows)[:, None]),
        0.0,
    )
    all_backs = lax.all_gather(own_back, "sp")
    rev_states = jnp.sum(reach[:, :, None, None] * all_backs, axis=0)[None]
    grad_proj = lax.psum_scatter(
        lax.dot_general(
            mixer_cot, mixer_out, (((0,), (0,)), ((), ())), preferred_element_type=jnp.float32
        ),
        "sp",
        scatter_dimension=0,
        tiled=True,
    )
    fwd_stack = entry_states
    grad_q = key_scale * jnp.einsum(
        "chij,cjhd->cihd", back_weights, span_key, preferred_element_type=jnp.float32
    )
    grad_q = grad_q + lead_decay[None, :, :, None] * jnp.einsum(
        "chde,cihe->cihd", fwd_stack, cot_wide, precision=lax.Precision.HIGHEST
    )
    grad_k = jnp.einsum(
        "chij,cihd->cjhd", back_weights, span_query, preferred_element_type=jnp.float32
    )
    grad_k = key_scale * (
        grad_k
        + tail_decay[None, :, :, None]
        * jnp.einsum("chde,cjhe->cjhd", rev_states, value_wide, precision=lax.Precision.HIGHEST)
    )
    grad_v = jnp.einsum(
        "chij,cihe->cjhe", fwd_weights, span_cot, preferred_element_type=jnp.float32
    )
    grad_v = grad_v + key_scale * tail_decay[None, :, :, None] * jnp.einsum(
        "chde,cjhd->cjhe", rev_states, key_wide, precision=lax.Precision.HIGHEST
    )
    flat_shape = (tok_rows, head_count * DK)
    return (
        grads[0],
        grads[1],
        grads[2],
        grad_proj,
        grad_q.reshape(flat_shape).astype(jnp.bfloat16),
        grad_k.reshape(flat_shape).astype(jnp.bfloat16),
        grad_v.reshape(flat_shape).astype(jnp.bfloat16),
    )


def solution(mesh):
    placed = (
        P("sp", None),
        P("sp", None),
        P("sp", None),
        P("sp", None),
        P("sp", None, "tp"),
        P("sp", None, "tp"),
        P("sp", "tp", None),
        P(None, "tp"),
        P("sp", "tp"),
        P("sp", "tp"),
        P("sp", "tp"),
        P("sp", "tp"),
        P("sp", "tp", None, None),
    )
    return jax.shard_map(
        per_device,
        mesh=mesh,
        in_specs=placed,
        out_specs=(
            P("sp", None, "tp"),
            P("sp", None, "tp"),
            P("sp", "tp", None),
            P("sp", "tp"),
            P("sp", "tp"),
            P("sp", "tp"),
            P("sp", "tp"),
        ),
        check_vma=False,
    )
```

```python
import functools
import math

import jax
import jax.numpy as jnp
from jax import lax
from jax.experimental import pallas as pl
from jax.experimental.pallas import tpu as pltpu
from jax.sharding import PartitionSpec as P

DK = 64
SPAN = 128
MESH = pl.DeviceIdType.MESH
VMEM = pl.BlockSpec(memory_space=pltpu.VMEM)


WAVE = (1, 4, 2, 5, 3, 6, 7)
HOPS = (2, 4, 6)
SPLIT = (6, 7)
PARTS = 4
NT = (((1,), (1,)), ((), ()))
TN = (((0,), (0,)), ((), ()))


def partner(me, k):
    for bit in (1, 2, 4):
        if k & bit:
            me = me + bit - 2 * bit * ((me // bit) % 2)
    return me


def wire(src, dst, send_sem, recv_sem, target):
    return pltpu.make_async_remote_copy(
        src_ref=src,
        dst_ref=dst,
        send_sem=send_sem,
        recv_sem=recv_sem,
        device_id=target,
        device_id_type=MESH,
    )


def send(src, dst, send_sem, recv_sem, target):
    copy = wire(src, dst, send_sem, recv_sem, target)
    copy.start()
    return copy


def greet(experts, me, tp, narrow):
    barrier = pltpu.get_barrier_semaphore()
    for k in range(1, experts):
        pl.semaphore_signal(
            barrier, inc=1, device_id={"sp": (me + k) % experts}, device_id_type=MESH
        )
    for k in range(1, narrow):
        pl.semaphore_signal(
            barrier, inc=1, device_id={"tp": (tp + k) % narrow}, device_id_type=MESH
        )
    return barrier, experts + narrow - 2


def rates_of(ids, total, tokens):
    half = total // 2
    ids = ids.astype(jnp.float32)
    fraction = jnp.minimum(ids, float(half)) * (1.0 / half)
    low, high = math.log(1.0 / 32.0), math.log(1.0 / tokens)
    base = jnp.exp((1.0 - fraction) * low + fraction * high)
    return base * (1.0 + jnp.maximum(ids - float(half), 0.0) * (1.0 / half))


def iota(shape, dim):
    return lax.broadcasted_iota(jnp.int32, shape, dim)


def dot(a, b, dims=None):
    if dims is None:
        dims = (((1,), (0,)), ((), ()))
    return lax.dot_general(a, b, dims, preferred_element_type=jnp.float32)


def mega_kernel(
    experts,
    narrow,
    routes_hbm,
    gains_hbm,
    rows_hbm,
    cot_hbm,
    gate_hbm,
    up_hbm,
    down_hbm,
    proj_hbm,
    query_hbm,
    key_hbm,
    value_hbm,
    out_hbm,
    entry_hbm,
    gg,
    gu,
    gd,
    grad_proj,
    grad_q,
    grad_k,
    grad_v,
    routes,
    gains,
    rows_in,
    cot_in,
    gate_w,
    up_w,
    down_w,
    gate_t,
    up_t,
    down_t,
    proj,
    query,
    key,
    value,
    entry,
    rows_s,
    cot_s,
    extra,
    rbuf,
    cbuf,
    place,
    share_w,
    act,
    dg,
    du,
    part,
    near_buf,
    side_out,
    side_in,
    far_out,
    back,
    mixer,
    all_out,
    all_mixer,
    state,
    given,
    all_state,
    l_in,
    s_sp, r_sp, s_y, r_y, s_c, r_c,
    s_n, r_n, s_s, r_s, s_f, r_f, s_g, r_g,
    s_r, r_r, s_m, r_m, s_h, r_h, s_b, r_b,
):
    me, tp = lax.axis_index("sp"), lax.axis_index("tp")
    core, row = tp % 2, tp // 2
    mate, across = tp + 1 - 2 * core, (tp + 2) % narrow
    mate_core = 1 - core
    barrier, count = greet(experts, me, tp, narrow)
    tok, width = rows_in.shape
    share = rows_s.shape[0] // experts
    cap = share * narrow
    cols = width // narrow
    pcols = width // experts
    heads = query.shape[1] // DK
    bf = jnp.bfloat16
    f32 = jnp.float32
    xmate = partner(me, 1)

    loads = {}
    first_in = (
        (9, rows_hbm, rows_in),
        (10, cot_hbm, cot_in),
        (3, out_hbm, all_out.at[me]),
        (0, gate_hbm.at[0], gate_w),
        (1, up_hbm.at[0], up_w),
        (2, down_hbm.at[0], down_w),
        (5, query_hbm, query),
        (6, key_hbm, key),
        (7, value_hbm, value),
        (8, entry_hbm.at[0], entry),
    )
    lanes = 128
    width = rows_in.shape[1]
    blocks = width // lanes
    held_at = [
        (spot // narrow) // 2 + 2 * ((spot // narrow) % 2) + narrow * (spot % narrow)
        for spot in range(blocks)
    ]
    first_in = first_in + tuple(
        (
            11 + spot,
            proj_hbm.at[lanes * block : lanes * (block + 1)],
            proj.at[lanes * spot : lanes * (spot + 1)],
        )
        for spot, block in enumerate(held_at)
    )
    def fetch(some):
        for i, src, dst in some:
            loads[i] = pltpu.make_async_copy(src, dst, l_in.at[i])
            loads[i].start()

    tables = [
        pltpu.make_async_copy(src, dst, l_in.at[11 + blocks + i])
        for i, (src, dst) in enumerate(((routes_hbm, routes), (gains_hbm, gains)))
    ]
    for copy in tables:
        copy.start()
    fetch(first_in[:2])
    for copy in tables:
        copy.wait()

    named = iota((tok, tok), 0)
    first, second = routes[0:1, :] == named, routes[1:2, :] == named
    hit = jnp.logical_or(first, second)
    before = jnp.where(iota((tok, tok), 0) < iota((tok, tok), 1), 1.0, 0.0).astype(bf)
    rank = dot(jnp.where(hit, 1.0, 0.0).astype(bf), before)
    spot = jnp.where(hit, rank, -1.0)
    place[...] = spot
    gain = jnp.where(first, gains[0:1, :], 0.0) + jnp.where(second, gains[1:2, :], 0.0)
    share_w[...] = gain

    def spread_rows(a):
        return jnp.broadcast_to(
            a[0:experts][:, None, :], (experts, share, tok)
        ).reshape(experts * share, tok)

    slot = (iota((experts * share, tok), 0) % share + share * tp).astype(f32)
    mask = jnp.where(spread_rows(spot) == slot, 1.0, 0.0)
    part_gain = jnp.sum(mask * spread_rows(gain), axis=1, keepdims=True)
    chosen = mask.astype(bf)
    loads[9].wait()
    loads[10].wait()
    rows_s[...] = dot(chosen, rows_in[...]).astype(bf)
    cot_s[...] = (part_gain * dot(chosen, cot_in[...])).astype(bf)
    def piece(buf, origin, index):
        return buf.at[pl.ds(pl.multiple_of(origin * cap + index * share, share), share)]

    def block(buf, index):
        return buf.at[pl.ds(pl.multiple_of(index * share, share), share)]

    def hold(origin):
        return pl.ds(pl.multiple_of(origin * cap, cap), cap)

    def quarter(index):
        return pl.ds(pl.multiple_of(index * cols, cols), cols)

    fetch(first_in[2:6])
    pl.semaphore_wait(barrier, count)
    arrays = ((rows_s, rbuf), (cot_s, cbuf))
    inner = jnp.logical_or(me // 2 == 1, me // 2 == 2)

    def lend(slot, block, hop):
        index = block ^ hop
        held = all_out.at[partner(me, block)]
        return wire(held, held, s_r.at[slot], r_r.at[index], {"sp": partner(me, hop)})

    far, side, near, relayed = {}, {}, {}, {}
    for k in WAVE:
        peer = partner(me, k)
        for a, (src, dst) in enumerate(arrays):
            far[a, k] = send(
                block(src, peer), piece(dst, me, tp), s_sp.at[a, k], r_sp.at[a, k], {"sp": peer}
            )
        if k == 3:
            loads[3].wait()
            lend(0, 0, 2).start()
    near_slot = (iota((share, tok), 0) + share * across).astype(f32)
    near_mask = jnp.where(place[pl.ds(xmate, 1), :] == near_slot, 1.0, 0.0)
    near_gain = jnp.sum(near_mask * share_w[pl.ds(xmate, 1), :], axis=1, keepdims=True)
    near_chosen = near_mask.astype(bf)
    extra[0] = dot(near_chosen, rows_in[...]).astype(bf)
    extra[1] = (near_gain * dot(near_chosen, cot_in[...])).astype(bf)
    own_slot = iota((cap, tok), 0).astype(f32)
    own_mask = jnp.where(place[pl.ds(me, 1), :] == own_slot, 1.0, 0.0)
    own_gain = jnp.sum(own_mask * share_w[pl.ds(me, 1), :], axis=1, keepdims=True)
    own_chosen = own_mask.astype(bf)

    for a, (_, dst) in enumerate(arrays):
        side[a, 1] = send(
            extra.at[a], piece(dst, me, across), s_y.at[a, 1], r_y.at[a, 1], {"sp": xmate}
        )
    rbuf[hold(me), :] = dot(own_chosen, rows_in[...]).astype(bf)
    cbuf[hold(me), :] = (own_gain * dot(own_chosen, cot_in[...])).astype(bf)

    def landed(block):
        held = all_out.at[me]
        wire(held, held, s_r.at[0], r_r.at[block], {"sp": xmate}).wait_recv()


    def land(k):
        origin = partner(me, k)
        for a, (_, dst) in enumerate(arrays):
            far[a, k].wait_recv()
            held = piece(dst, origin, tp)
            if k > 1:
                side[a, k] = send(held, held, s_y.at[a, k], r_y.at[a, k], {"tp": across})
            near[a, k] = send(held, held, s_c.at[a, 0, k], r_c.at[a, 0, k], {"tp": mate})

    def relay(k):
        origin = partner(me, k)
        for a, (_, dst) in enumerate(arrays):
            side[a, k].wait_recv()
            held = piece(dst, origin, across)
            relayed[a, k] = send(held, held, s_c.at[a, 1, k], r_c.at[a, 1, k], {"tp": mate})

    def parting(k, half):
        return wire(
            part.at[hold(partner(me, k)), quarter(half * 2 + mate_core)],
            near_buf.at[k, half],
            s_n.at[k, half],
            r_n.at[k, half],
            {"tp": mate},
        )

    def chunk(ks):
        for k in ks:
            if k > 0:
                for a in range(2):
                    near[a, k].wait_recv()
                    relayed[a, k].wait_recv()
        size = len(ks) * cap
        at = pl.ds(pl.multiple_of(partner(me, ks[0]) // len(ks) * size, size), size)
        rows, cots = rbuf[at, :], cbuf[at, :]
        gate = dot(rows, gate_w[...])
        up = dot(rows, up_w[...])
        sig = jax.nn.sigmoid(gate)
        d_act = dot(cots, down_t[...])
        act[at, :] = (gate * sig * up).astype(bf)
        d_gate = (d_act * up * sig * (1.0 + gate * (1.0 - sig))).astype(bf)
        d_up = (d_act * gate * sig).astype(bf)
        dg[at, :] = d_gate
        du[at, :] = d_up
        sums = (dot(d_gate, gate_t[...]) + dot(d_up, up_t[...])).astype(bf)
        for spot, block in enumerate(held_at):
            part[at, lanes * spot : lanes * (spot + 1)] = sums[
                :, lanes * block : lanes * (block + 1)
            ]
        for k in ks:
            for half in range(2):
                parting(k, half).start()

    crossed, gone = {}, {}

    split = cols // PARTS
    sides = tuple(range(PARTS))

    def halves(k):
        return sides if k in SPLIT else (None,)

    def span(half, base=None):
        start = 0 if half is None else half * split
        size = cols if half is None else split
        if base is None:
            return slice(start, start + size)
        return pl.ds(pl.multiple_of(base + start, size), size)

    def cross(k, half=None):
        dest = partner(me, k)
        index = half or 0
        if index == 0:
            parting(k, 0).wait_recv()
            parting(k, 1).wait_recv()
        at = span(half)
        side_out[k, :, at] = (
            part[hold(dest), span(half, across * cols)].astype(f32)
            + near_buf.at[k, 1 - row][:, at].astype(f32)
        ).astype(bf)
        crossed[k, half] = send(
            side_out.at[k, :, at],
            side_in.at[k, :, at],
            s_s.at[k, index],
            r_s.at[k, index],
            {"tp": across},
        )

    def ship(k, half=None):
        dest = partner(me, k)
        index = half or 0
        crossed[k, half].wait_recv()
        at = span(half)
        done = (
            part[hold(dest), span(half, tp * cols)].astype(f32)
            + near_buf.at[k, row][:, at].astype(f32)
            + side_in.at[k][:, at].astype(f32)
        ).astype(bf)
        if k == 0:
            back[me] = done
        else:
            far_out[k, :, at] = done
            gone[k, half] = send(
                far_out.at[k, :, at],
                back.at[me, :, at],
                s_f.at[k, index],
                r_f.at[k, index],
                {"sp": dest},
            )

    def weight_grads(step):
        span = width // experts
        at = pl.ds(step * span, span)
        rows = rbuf[:, at]
        gg[at, :] = dot(rows, dg[...], TN).astype(bf)
        gu[at, :] = dot(rows, du[...], TN).astype(bf)
        gd[:, at] = dot(act[...], cbuf[:, at], TN).astype(bf)

    def early(when):
        @pl.when(when)
        def _():
            chunk((0, 1, 2, 3))

    def crossout():
        landed(2)
        lend(1, 0, 1).start()
        lend(2, 2, 1).start()

        @pl.when(inner)
        def _():
            lend(3, 0, 6).start()
            lend(4, 2, 6).start()

    def returnout():
        @pl.when(inner)
        def _():
            landed(6)
            landed(4)
            lend(3 + 2, 6, 2).start()
            lend(3 + 3, 4, 2).start()

    fetch(first_in[6:])
    turned = jnp.transpose(place[...])
    lane = iota((tok, 2 * cap), 1)
    picks = jnp.concatenate(
        [
            jnp.where(
                jnp.where(lane < cap, turned[:, 2 * p : 2 * p + 1], turned[:, 2 * p + 1 : 2 * p + 2])
                == (lane % cap).astype(f32),
                1.0,
                0.0,
            ).astype(bf)
            for p in range(experts // 2)
        ],
        axis=1,
    )
    for i in (0, 1, 2):
        loads[i].wait()
    for tile in range(experts):
        at = slice(tile * pcols, (tile + 1) * pcols)
        gate_t[:, at] = jnp.transpose(gate_w[at, :])
        up_t[:, at] = jnp.transpose(up_w[at, :])
        down_t[at, :] = jnp.transpose(down_w[:, at])
    land(1)
    land(4)
    land(2)
    relay(4)
    land(5)
    relay(2)
    land(3)
    relay(5)
    chunk((4, 5))
    relay(3)
    relay(1)
    cross(4)
    cross(5)
    chunk((0, 1, 2, 3))
    land(6)
    land(7)
    cross(2)
    cross(3)
    cross(1)
    cross(0)
    ship(4)
    ship(5)
    crossout()
    relay(6)
    relay(7)
    chunk((6, 7))
    ship(2)
    ship(3)
    cross(6, 0)
    cross(7, 0)
    cross(6, 1)
    cross(7, 1)
    cross(6, 2)
    cross(7, 2)
    cross(6, 3)
    cross(7, 3)
    weight_grads(0)
    ship(1)
    weight_grads(1)
    ship(0)
    ship(6, 0)
    ship(7, 0)
    ship(6, 1)
    ship(7, 1)
    ship(6, 2)
    ship(7, 2)
    ship(6, 3)
    ship(7, 3)
    returnout()
    weight_grads(2)
    weight_grads(3)
    is_hub = core == me % 2

    def toward(m):
        dest = 2 * m + core
        at = pl.ds(pl.multiple_of(tp * cols + m * lanes, lanes), lanes)
        copy = wire(mixer.at[:, at], all_mixer.at[row, me], s_m.at[m], r_m.at[me], {"sp": dest})
        return dest, at, copy

    def strip(index, half):
        return mixer.at[:, span(half, index * cols)]

    def give(half, way):
        mine = strip(tp, half)
        return wire(mine, mine, s_g.at[half, way], r_g.at[half, way], {"tp": (across, mate)[way]})

    def regive(half):
        held = strip(across, half)
        return wire(held, held, s_g.at[half, 2], r_g.at[half, 2], {"tp": mate})

    for half in sides:
        for k in WAVE:
            if k in SPLIT:
                gone[k, half].wait_recv()
            elif half == 0:
                gone[k, None].wait_recv()
        slots = back[:, :, half * split : (half + 1) * split].reshape(experts * cap, split)
        gained = dot(picks, slots)
        for n in range(narrow // PARTS):
            m = half * (narrow // PARTS) + n
            block = pl.multiple_of((narrow * m + 2 * core + row) * lanes, lanes)
            spot = pl.multiple_of(tp * cols + m * lanes, lanes)
            mixer[:, pl.ds(spot, lanes)] = (
                cot_in[:, pl.ds(block, lanes)].astype(f32)
                + gained[:, lanes * n : lanes * (n + 1)]
            ).astype(bf)
        give(half, 0).start()
        give(half, 1).start()
        for n in range(narrow // PARTS):
            m = half * (narrow // PARTS) + n
            dest, at, copy = toward(m)

            @pl.when(dest != me)
            def _():
                copy.start()

            @pl.when(dest == me)
            def _():
                all_mixer[row, me] = mixer[:, at]

    for i in range(11, 11 + blocks):
        loads[i].wait()
    for half in sides:
        give(half, 1).wait_recv()

    def heads_of(side):
        at = pl.ds(pl.multiple_of(side * 2 * cols, 2 * cols), 2 * cols)
        return dot(mixer[:, at], proj[at, :])

    def quarter_heads(index):
        return dot(mixer[:, quarter(index)], proj[quarter(index), :])

    raw = heads_of(row)
    for half in sides:
        give(half, 0).wait_recv()
        regive(half).start()
    raw = raw + quarter_heads(across)
    for i in (5, 6, 7, 8):
        loads[i].wait()
    for half in sides:
        regive(half).wait_recv()

    raw = raw + quarter_heads(narrow - 1 - tp)
    positions = (iota((tok, 2 * DK), 0)).astype(f32)
    lane = iota((tok, 2 * DK), 1)
    low = lane < DK
    all_heads = heads * narrow
    tokens = tok * experts
    scale = DK ** (-0.5)
    pairs = heads // 2
    cots, rate = [], []
    for p in range(pairs):
        ids = tp * heads + 2 * p + iota((1, 2 * DK), 1) // DK
        r = rates_of(ids, all_heads, tokens)
        rate.append(r)
        at = slice(2 * DK * p, 2 * DK * (p + 1))
        here = positions + (me * tok + 1).astype(f32)
        norm = jnp.sqrt((1.0 - jnp.exp(-2.0 * r)) / (1.0 - jnp.exp(-2.0 * r * here)))
        cot = (raw[:, at] * norm).astype(bf)
        cots.append(cot)
        lead = jnp.exp(-r * (positions + 1.0))
        lead_q = (query[:, at].astype(f32) * lead).astype(bf)
        both = dot(lead_q, cot, TN)
        state[DK * p : DK * (p + 1), :] = jnp.where(
            low[0:DK], both[0:DK, :], both[DK : 2 * DK, :]
        ).astype(bf)
    def hop(k):
        return wire(state, all_state.at[k // 2], s_b.at[k // 2], r_b.at[k // 2], {"sp": partner(me, k)})

    for k in HOPS:

        @pl.when(partner(me, k) < me)
        def _():
            hop(k).start()

    @pl.when(jnp.logical_not(inner))
    def _():
        landed(4)
        landed(6)

    lend(7, 4, 1).start()
    lend(8, 6, 1).start()
    distance = (iota((tok, tok), 0) - iota((tok, tok), 1)).astype(f32)
    q_part, k_part, v_part = [], [], []
    zero = jnp.zeros((tok, 2 * DK), bf)
    shift = jnp.where(iota((DK, 2 * DK), 1) == iota((DK, 2 * DK), 0) + DK, 1.0, 0.0).astype(bf)
    keep = jnp.where(iota((DK, 2 * DK), 1) == iota((DK, 2 * DK), 0), 1.0, 0.0).astype(bf)
    for p in range(pairs):
        at = slice(2 * DK * p, 2 * DK * (p + 1))
        q, k_, v, cot = query[:, at], key[:, at], value[:, at], cots[p]
        gq = jnp.zeros((tok, 2 * DK), f32)
        gk = jnp.zeros((tok, 2 * DK), f32)
        gv = jnp.zeros((tok, 2 * DK), f32)
        for half in range(2):
            pick = low if half == 0 else jnp.logical_not(low)
            r = rates_of(tp * heads + 2 * p + half + iota((1, tok), 1) * 0, all_heads, tokens)
            down = jnp.where(distance >= 0, jnp.exp(-r * jnp.maximum(distance, 0.0)), 0.0)
            over = jnp.where(distance <= 0, jnp.exp(-r * jnp.maximum(-distance, 0.0)), 0.0)
            qh, kh = jnp.where(pick, q, zero), jnp.where(pick, k_, zero)
            vh, ch = jnp.where(pick, v, zero), jnp.where(pick, cot, zero)
            back_w = (dot(cot, vh, NT) * down).astype(bf)
            back_t = (dot(vh, cot, NT) * over).astype(bf)
            fwd_t = (dot(kh, q, NT) * scale * over).astype(bf)
            gq = gq + dot(back_w, kh)
            gk = gk + dot(back_t, qh)
            gv = gv + dot(fwd_t, ch)
        lead = jnp.exp(-rate[p] * (positions + 1.0))
        upper = dot(entry[2 * p].astype(bf), keep)
        lower = dot(entry[2 * p + 1].astype(bf), shift)
        held = jnp.concatenate([upper, lower], axis=0).astype(bf)
        gq = scale * gq + lead * dot(cot, held, NT)
        grad_q[:, at] = gq.astype(bf)
        k_part.append(gk)
        v_part.append(gv)

    def handover(i):
        held = all_mixer.at[row, i]
        return wire(held, held, s_h.at[0, i], r_h.at[0, i], {"tp": across})

    def handoff(half, i):
        held = all_mixer.at[half, i]
        return wire(held, held, s_h.at[1 + half, i], r_h.at[1 + half, i], {"tp": mate})

    def arrival(i):
        held = all_mixer.at[row, i]
        return wire(held, held, s_m.at[0], r_m.at[i], {"tp": mate})

    @pl.when(is_hub)
    def _():
        for k in (0,) + WAVE:
            i = partner(me, k)
            if k > 0:
                arrival(i).wait_recv()
            handover(i).start()
            handoff(row, i).start()

    weight_grads(4)
    weight_grads(5)
    weight_grads(6)
    weight_grads(7)
    for k in HOPS:

        @pl.when(partner(me, k) > me)
        def _():
            hop(k).wait_recv()

    def gathered(p, target):
        total = jnp.zeros((DK, 2 * DK), f32)
        for k in HOPS:
            ahead = partner(me, k) - target - 1
            reach = jnp.exp(-rate[p] * (jnp.maximum(ahead, 0) * tok).astype(f32))
            held = all_state[k // 2, DK * p : DK * (p + 1), :].astype(f32)
            due = iota((DK, 2 * DK), 0) * 0 + partner(me, k) > me
            total = total + jnp.where(due, reach * held, 0.0)
        return total

    ahead_of_mate = jnp.where(me > xmate, 1.0, 0.0)
    for p in range(pairs):
        at = slice(DK * p, DK * (p + 1))
        given[at, :] = (gathered(p, xmate) + ahead_of_mate * state[at, :].astype(f32)).astype(bf)
    pass_on = send(given, all_state.at[0], s_b.at[0], r_b.at[0], {"sp": xmate})

    @pl.when(is_hub)
    def _():
        for k in (0,) + WAVE:
            i = partner(me, k)
            handover(i).wait_recv()
            handoff(1 - row, i).start()

    @pl.when(jnp.logical_not(is_hub))
    def _():
        for half in range(2):
            for i in range(experts):
                handoff(half, i).wait_recv()

    for block in (1, 3, 5, 7):
        landed(block)
    for half in range(2):
        at = slice(half * (pcols // 2), (half + 1) * (pcols // 2))
        grad_proj[at, :] = dot(
            all_mixer[half].reshape(experts * tok, pcols // 2),
            all_out[...].reshape(experts * tok, all_out.shape[2]),
            TN,
        )
    pass_on.wait_recv()
    for p in range(pairs):
        at = slice(2 * DK * p, 2 * DK * (p + 1))
        later = gathered(p, me) + all_state[0, DK * p : DK * (p + 1), :].astype(f32)
        whole = jnp.concatenate(
            [jnp.where(low[0:DK], later, 0.0), jnp.where(low[0:DK], 0.0, later)], axis=0
        ).astype(bf)
        tail = jnp.exp(-rate[p] * (tok - 1.0 - positions))
        grad_k[:, at] = (scale * (k_part[p] + tail * dot(value[:, at], whole, NT))).astype(bf)
        grad_v[:, at] = (v_part[p] + scale * tail * dot(key[:, at], whole)).astype(bf)

    for group in (far, side, near, relayed, crossed, gone):
        for copy in group.values():
            copy.wait_send()
    for k in range(experts):
        for half in range(2):
            parting(k, half).wait_send()
    for half in sides:
        give(half, 0).wait_send()
        give(half, 1).wait_send()
        regive(half).wait_send()
    pass_on.wait_send()
    for slot, block, step in ((0, 0, 2), (1, 0, 1), (2, 2, 1), (7, 4, 1), (8, 6, 1)):
        lend(slot, block, step).wait_send()

    @pl.when(inner)
    def _():
        for slot, block, step in ((3, 0, 6), (4, 2, 6), (5, 6, 2), (6, 4, 2)):
            lend(slot, block, step).wait_send()

    for k in HOPS:

        @pl.when(partner(me, k) < me)
        def _():
            hop(k).wait_send()

    for m in range(narrow):
        dest, at, copy = toward(m)

        @pl.when(dest != me)
        def _():
            copy.wait_send()

    @pl.when(is_hub)
    def _():
        for i in range(experts):
            handover(i).wait_send()
            handoff(0, i).wait_send()
            handoff(1, i).wait_send()


def settle_kernel(count, *refs):
    sources, targets, done = refs[:count], refs[count : 2 * count], refs[2 * count]
    copies = []
    for i in range(count):
        target = targets[i]
        if len(target.shape) > len(sources[i].shape):
            target = target.at[0]
        copies.append(pltpu.make_async_copy(sources[i], target, done.at[i]))
    for copy in copies:
        copy.start()
    for copy in copies:
        copy.wait()


def settle(arrays, shapes):
    count = len(arrays)
    return pl.pallas_call(
        functools.partial(settle_kernel, count),
        out_shape=tuple(jax.ShapeDtypeStruct(s, a.dtype) for s, a in zip(shapes, arrays)),
        in_specs=[pl.BlockSpec(memory_space=pl.ANY)] * count,
        out_specs=(pl.BlockSpec(memory_space=pl.ANY),) * count,
        scratch_shapes=[pltpu.SemaphoreType.DMA((count,))],
        compiler_params=pltpu.CompilerParams(vmem_limit_bytes=1024 * 1024),
    )(*arrays)


def mega(routes, gains, rows, cot, gate, up, down, proj, query, key, value, out, entry, experts, narrow):
    tok, width = rows.shape
    top = routes.shape[0]
    cap = 2 * tok * top // experts
    share = cap // narrow
    hidden = gate.shape[2]
    hv = query.shape[1]
    cols, pcols = width // narrow, width // experts
    heads = hv // DK
    bf, f32 = jnp.bfloat16, jnp.float32
    sem = pltpu.SemaphoreType.DMA
    any_spec = pl.BlockSpec(memory_space=pl.ANY)
    n = experts
    v = pltpu.VMEM
    results = pl.pallas_call(
        functools.partial(mega_kernel, experts, narrow),
        out_shape=(
            v(gate.shape[1:], bf),
            v(up.shape[1:], bf),
            v(down.shape[1:], bf),
            v((pcols, hv), f32),
            v(query.shape, bf),
            v(query.shape, bf),
            v(query.shape, bf),
        ),
        in_specs=[pl.BlockSpec(memory_space=pltpu.HBM)] * 13,
        out_specs=(VMEM,) * 7,
        scratch_shapes=[
            v(routes.shape, jnp.int32),
            v(gains.shape, f32),
            v((tok, width), bf),
            v((tok, width), bf),
            v((width, hidden), bf),
            v((width, hidden), bf),
            v((hidden, width), bf),
            v((hidden, width), bf),
            v((hidden, width), bf),
            v((width, hidden), bf),
            v((width, hv), bf),
            v((tok, hv), bf),
            v((tok, hv), bf),
            v((tok, hv), bf),
            v((heads, DK, DK), f32),
            v((n * share, width), bf),
            v((n * share, width), bf),
            v((2, share, width), bf),
            v((n * cap, width), bf),
            v((n * cap, width), bf),
            v((tok, tok), f32),
            v((tok, tok), f32),
            v((n * cap, hidden), bf),
            v((n * cap, hidden), bf),
            v((n * cap, hidden), bf),
            v((n * cap, width), bf),
            v((n, 2, cap, cols), bf),
            v((n, cap, cols), bf),
            v((n, cap, cols), bf),
            v((n, cap, cols), bf),
            v((n, cap, cols), bf),
            v((tok, width), bf),
            v((n, tok, hv), bf),
            v((2, n, tok, pcols // 2), bf),
            v((heads // 2 * DK, 2 * DK), bf),
            v((heads // 2 * DK, 2 * DK), bf),
            v((n // 2, heads // 2 * DK, 2 * DK), bf),
            sem((13 + width // 128,)),
            sem((2, n)), sem((2, n)), sem((2, n)), sem((2, n)), sem((2, 2, n)), sem((2, 2, n)),
            sem((n, 2)), sem((n, 2)), sem((n, PARTS)), sem((n, PARTS)), sem((n, PARTS)), sem((n, PARTS)), sem((PARTS, 3)), sem((PARTS, 3)),
            sem((9,)), sem((n,)), sem((narrow,)), sem((n,)), sem((3, n)), sem((3, n)), sem((n // 2,)), sem((n // 2,)),
        ],
        compiler_params=pltpu.CompilerParams(
            collective_id=0, has_side_effects=True, vmem_limit_bytes=62800000
        ),
    )(routes, gains, rows, cot, gate, up, down, proj, query, key, value, out, entry)
    flat = (tok, hv)
    return settle(results, (gate.shape, up.shape, down.shape, (pcols, hv), flat, flat, flat))


def decay_rates(head_ids, head_count, token_count):
    half_count = head_count // 2
    fraction = jnp.minimum(head_ids, half_count) / half_count
    base_rate = jnp.exp(
        (1.0 - fraction) * jnp.log(1.0 / 32.0) + fraction * jnp.log(1.0 / token_count)
    )
    return base_rate * (1.0 + jnp.maximum(head_ids - half_count, 0.0) / half_count)


def position_norm(positions, head_rates):
    return jnp.sqrt(
        jnp.expm1(-2.0 * head_rates)[None, :]
        / jnp.expm1(-2.0 * head_rates[None, :] * (positions[:, None] + 1.0))
    )


def expert_grads(exp_rows, exp_cot, activated, d_gate, d_up):
    row_dims = (((0,), (0,)), ((), ()))
    grad_gate = lax.dot_general(
        exp_rows, d_gate, row_dims, preferred_element_type=jnp.float32
    ).astype(jnp.bfloat16)
    grad_up = lax.dot_general(exp_rows, d_up, row_dims, preferred_element_type=jnp.float32).astype(
        jnp.bfloat16
    )
    grad_down = lax.dot_general(
        activated, exp_cot, row_dims, preferred_element_type=jnp.float32
    ).astype(jnp.bfloat16)
    return (grad_gate[None], grad_up[None], grad_down[None])


def per_device(
    layer_input,
    out_cot,
    routes,
    route_weights,
    gate_weights,
    up_weights,
    down_weights,
    out_proj,
    queries,
    keys,
    values,
    mixer_out,
    entry_states,
):
    tok_rows, model_width = layer_input.shape
    experts = lax.axis_size("sp")
    narrow = lax.axis_size("tp")
    top_count = routes.shape[1]
    hidden, hv = gate_weights.shape[2], queries.shape[1]
    fits = top_count == 2 and tok_rows == SPAN and narrow == 4 and experts == 8
    fits = fits and 2 * tok_rows * top_count == experts * 64 and hidden % 128 == 0
    if fits and model_width % (experts * 256) == 0 and hv % 128 == 0:
        return mega(
            routes.T,
            route_weights.T,
            layer_input,
            out_cot,
            gate_weights,
            up_weights,
            down_weights,
            out_proj,
            queries,
            keys,
            values,
            mixer_out,
            entry_states,
            experts,
            narrow,
        )
    pair_count = tok_rows * top_count
    capacity = 2 * pair_count // experts
    flat_routes = routes.reshape(pair_count)
    onehot = (flat_routes[:, None] == jnp.arange(experts, dtype=jnp.int32)[None, :]).astype(
        jnp.int32
    )
    earlier = jnp.cumsum(onehot, axis=0) - onehot
    target = flat_routes * capacity + jnp.sum(earlier * onehot, axis=1)
    share = capacity // narrow
    first_row = lax.axis_index("tp") * share
    owner_tok = jnp.arange(pair_count, dtype=jnp.int32) // top_count
    slot_tok = jnp.full((experts * capacity,), tok_rows, jnp.int32).at[target].set(owner_tok)
    slot_weight = (
        jnp.zeros((experts * capacity,), jnp.float32)
        .at[target]
        .set(route_weights.reshape(pair_count))
    )
    blank_row = jnp.zeros((1, model_width), jnp.bfloat16)
    sent_rows = jnp.concatenate([layer_input, blank_row], 0)[slot_tok].reshape(
        experts, capacity, model_width
    )
    picked_cot = jnp.concatenate([out_cot, blank_row], 0)[slot_tok]
    sent_cot = (
        (slot_weight[:, None] * picked_cot.astype(jnp.float32))
        .astype(jnp.bfloat16)
        .reshape(experts, capacity, model_width)
    )
    part_rows = lax.dynamic_slice_in_dim(sent_rows, first_row, share, 1)
    part_cot = lax.dynamic_slice_in_dim(sent_cot, first_row, share, 1)
    got_rows, got_cot = (
        lax.all_to_all(part_rows, "sp", split_axis=0, concat_axis=0, tiled=True),
        lax.all_to_all(part_cot, "sp", split_axis=0, concat_axis=0, tiled=True),
    )
    got_rows, got_cot = (
        lax.all_gather(got_rows, "tp", axis=1, tiled=True),
        lax.all_gather(got_cot, "tp", axis=1, tiled=True),
    )
    exp_rows = got_rows.reshape(experts * capacity, model_width)
    exp_cot = got_cot.reshape(experts * capacity, model_width)
    gate_w = gate_weights[0]
    up_w = up_weights[0]
    down_w = down_weights[0]
    gate_pre = jnp.dot(exp_rows, gate_w, preferred_element_type=jnp.float32)
    up_pre = jnp.dot(exp_rows, up_w, preferred_element_type=jnp.float32)
    sigmoid_g = jax.nn.sigmoid(gate_pre)
    activated = (gate_pre * sigmoid_g * up_pre).astype(jnp.bfloat16)
    width_dims = (((1,), (1,)), ((), ()))
    d_act = lax.dot_general(exp_cot, down_w, width_dims, preferred_element_type=jnp.float32)
    d_gate = (d_act * up_pre * sigmoid_g * (1.0 + gate_pre * (1.0 - sigmoid_g))).astype(
        jnp.bfloat16
    )
    d_up = (d_act * gate_pre * sigmoid_g).astype(jnp.bfloat16)
    grads = expert_grads(exp_rows, exp_cot, activated, d_gate, d_up)
    partial_sum = lax.dot_general(d_gate, gate_w, width_dims, preferred_element_type=jnp.float32)
    partial_sum = partial_sum + lax.dot_general(
        d_up, up_w, width_dims, preferred_element_type=jnp.float32
    )
    summed = lax.psum_scatter(
        partial_sum.reshape(experts, capacity, model_width), "tp", scatter_dimension=2, tiled=True
    )
    returned = lax.all_to_all(
        summed.astype(jnp.bfloat16), "sp", split_axis=0, concat_axis=0, tiled=True
    )
    col_count = model_width // narrow
    first_col = lax.axis_index("tp") * col_count
    back_flat = returned.reshape(experts * capacity, col_count)
    pair_back = back_flat[target].reshape(tok_rows, top_count, col_count).astype(jnp.float32)
    own_cols = lax.dynamic_slice_in_dim(out_cot, first_col, col_count, 1).astype(jnp.float32)
    cot_cols = (own_cols + jnp.sum(pair_back, axis=1)).astype(jnp.bfloat16)
    mixer_cot = lax.all_gather(cot_cols, "tp", axis=1, tiled=True)
    head_count = queries.shape[1] // DK
    head_ids = (lax.axis_index("tp") * head_count + jnp.arange(head_count, dtype=jnp.int32)).astype(
        jnp.float32
    )
    head_rates = decay_rates(head_ids, head_count * narrow, tok_rows * experts)
    positions = (lax.axis_index("sp") * tok_rows + jnp.arange(tok_rows, dtype=jnp.int32)).astype(
        jnp.float32
    )
    head_cot = jnp.dot(mixer_cot, out_proj, preferred_element_type=jnp.float32).reshape(
        tok_rows, head_count, DK
    )
    head_cot = (head_cot * position_norm(positions, head_rates)[:, :, None]).astype(jnp.bfloat16)
    span_count = tok_rows // SPAN
    span_shape = (span_count, SPAN, head_count, DK)
    span_query = queries.reshape(span_shape)
    span_key = keys.reshape(span_shape)
    span_value = values.reshape(span_shape)
    span_cot = head_cot.reshape(span_shape)
    key_scale = DK ** (-0.5)
    offsets = jnp.arange(SPAN, dtype=jnp.float32)
    distance = offsets[:, None] - offsets[None, :]
    decay_mat = jnp.where(
        distance[None] >= 0,
        jnp.exp(-head_rates[:, None, None] * jnp.maximum(distance, 0.0)[None]),
        0.0,
    )
    fwd_weights = (
        jnp.einsum("cihd,cjhd->chij", span_query, span_key, preferred_element_type=jnp.float32)
        * key_scale
        * decay_mat[None]
    ).astype(jnp.bfloat16)
    back_weights = (
        jnp.einsum("cihd,cjhd->chij", span_cot, span_value, preferred_element_type=jnp.float32)
        * decay_mat[None]
    ).astype(jnp.bfloat16)
    tail_decay = jnp.exp(-head_rates[None, :] * (SPAN - 1.0 - offsets)[:, None])
    lead_decay = jnp.exp(-head_rates[None, :] * (offsets + 1.0)[:, None])
    query_wide = span_query.astype(jnp.float32)
    key_wide = span_key.astype(jnp.float32)
    value_wide = span_value.astype(jnp.float32)
    cot_wide = span_cot.astype(jnp.float32)
    backs = jnp.einsum(
        "cihd,cihe->chde",
        query_wide * lead_decay[None, :, :, None],
        cot_wide,
        precision=lax.Precision.HIGHEST,
    )
    own_back = backs[0]
    ahead = jnp.arange(experts, dtype=jnp.int32) - lax.axis_index("sp") - 1
    reach = jnp.where(
        ahead[:, None] >= 0,
        jnp.exp(-head_rates[None, :] * (jnp.maximum(ahead, 0) * tok_rows)[:, None]),
        0.0,
    )
    all_backs = lax.all_gather(own_back, "sp")
    rev_states = jnp.sum(reach[:, :, None, None] * all_backs, axis=0)[None]
    grad_proj = lax.psum_scatter(
        lax.dot_general(
            mixer_cot, mixer_out, (((0,), (0,)), ((), ())), preferred_element_type=jnp.float32
        ),
        "sp",
        scatter_dimension=0,
        tiled=True,
    )
    fwd_stack = entry_states
    grad_q = key_scale * jnp.einsum(
        "chij,cjhd->cihd", back_weights, span_key, preferred_element_type=jnp.float32
    )
    grad_q = grad_q + lead_decay[None, :, :, None] * jnp.einsum(
        "chde,cihe->cihd", fwd_stack, cot_wide, precision=lax.Precision.HIGHEST
    )
    grad_k = jnp.einsum(
        "chij,cihd->cjhd", back_weights, span_query, preferred_element_type=jnp.float32
    )
    grad_k = key_scale * (
        grad_k
        + tail_decay[None, :, :, None]
        * jnp.einsum("chde,cjhe->cjhd", rev_states, value_wide, precision=lax.Precision.HIGHEST)
    )
    grad_v = jnp.einsum(
        "chij,cihe->cjhe", fwd_weights, span_cot, preferred_element_type=jnp.float32
    )
    grad_v = grad_v + key_scale * tail_decay[None, :, :, None] * jnp.einsum(
        "chde,cjhd->cjhe", rev_states, key_wide, precision=lax.Precision.HIGHEST
    )
    flat_shape = (tok_rows, head_count * DK)
    return (
        grads[0],
        grads[1],
        grads[2],
        grad_proj,
        grad_q.reshape(flat_shape).astype(jnp.bfloat16),
        grad_k.reshape(flat_shape).astype(jnp.bfloat16),
        grad_v.reshape(flat_shape).astype(jnp.bfloat16),
    )


def solution(mesh):
    placed = (
        P("sp", None),
        P("sp", None),
        P("sp", None),
        P("sp", None),
        P("sp", None, "tp"),
        P("sp", None, "tp"),
        P("sp", "tp", None),
        P(None, "tp"),
        P("sp", "tp"),
        P("sp", "tp"),
        P("sp", "tp"),
        P("sp", "tp"),
        P("sp", "tp", None, None),
    )
    return jax.shard_map(
        per_device,
        mesh=mesh,
        in_specs=placed,
        out_specs=(
            P("sp", None, "tp"),
            P("sp", None, "tp"),
            P("sp", "tp", None),
            P("sp", "tp"),
            P("sp", "tp"),
            P("sp", "tp"),
            P("sp", "tp"),
        ),
        check_vma=False,
    )
```
